32 devices in a mesh: fs: 4 (over z), rep: 4 (over y, x), tp: 2 (over core).
Axes of the slice: x: 2, y: 2, z: 4, core: 2. Of those that a mesh axis runs over, the one named last changes fastest.
Arguments:
- query_input: bfloat16 [16384, 4096], P(('fs', 'rep')), may hold values from -6 to 6
- query_cotangent: bfloat16 [16384, 1024], P(('fs', 'rep'), 'tp'), may hold values from -0.046875 to 0.046875
- branch_output: bfloat16 [16384, 2048], P(('fs', 'rep')), may hold values from -6 to 6
- layer_cotangent: bfloat16 [16384, 4096], P(('fs', 'rep'), 'tp'), may hold values from -0.046875 to 0.046875
- query_weight: float32 [4096, 1024], P(('rep', 'fs'), 'tp'), may hold values from -0.09375 to 0.09375
- output_weight: float32 [2048, 4096], P(('rep', 'fs'), 'tp'), may hold values from -0.125 to 0.125
- query_basis: bfloat16 [4096, 512], P(('rep', 'fs')), may hold values from -0.09375 to 0.09375
- output_basis: bfloat16 [2048, 512], P(('rep', 'fs')), may hold values from -0.125 to 0.125
- query_first: float32 [512, 1024], P(('rep', 'fs'), 'tp'), may hold values from -20 to 20
- query_second: float32 [512, 1024], P(('rep', 'fs'), 'tp'), may hold values from 0.25 to 2
- output_first: float32 [512, 4096], P(('rep', 'fs'), 'tp'), may hold values from -20 to 20
- output_second: float32 [512, 4096], P(('rep', 'fs'), 'tp'), may hold values from 0.25 to 2
Outputs:
- query_update: float32 [4096, 1024], P(('rep', 'fs'), 'tp')
- output_update: float32 [2048, 4096], P(('rep', 'fs'), 'tp')
- query_first_next: float32 [512, 1024], P(('rep', 'fs'), 'tp')
- query_second_next: float32 [512, 1024], P(('rep', 'fs'), 'tp')
- output_first_next: float32 [512, 4096], P(('rep', 'fs'), 'tp')
- output_second_next: float32 [512, 4096], P(('rep', 'fs'), 'tp')
- query_copy: bfloat16 [4096, 1024], P('rep', 'tp')
- output_copy: bfloat16 [2048, 4096], P('rep', 'tp')
The draws below stay inside these ranges and needn't reach their ends.
All inputs are finite; a program needn't handle non-finite values.
Results may differ from the reference program's by a relative error of at most 0.0055.
Values may be sent and summed in bfloat16 or wider, within the bound.
A program may use at most 128 MiB of HBM per device.

```python
import math
import jax
import jax.numpy as jnp
from jax import lax

D = 4096
QKW = 1024
VW = 2048
R = 512
TOKENS = 16384


def first_moment(key, rows, cols):
    row_scale = 0.3 * 10.0 ** (jnp.arange(rows, dtype=jnp.float32) / (rows - 1))
    col_scale = jnp.exp(jax.random.uniform(jax.random.fold_in(key, 7), (cols,), jnp.float32, -0.7, 0.7))
    base = jnp.clip(jax.random.normal(jax.random.fold_in(key, 11), (rows, cols), jnp.float32), -3.0, 3.0)
    return base * row_scale[:, None] * col_scale[None, :]


def draw_query_first(key, part):
    return first_moment(key, R, QKW)


def draw_output_first(key, part):
    return first_moment(key, R, D)


def level_of(stream_key, extent, split, low, high):
    def one(dim, blocks):
        heights = jax.random.uniform(jax.random.fold_in(jax.random.fold_in(stream_key, 6), dim), (blocks,), jnp.float32, low / len(split), high / len(split))
        return jnp.repeat(jnp.exp(heights), extent[dim] // blocks).reshape((-1,) + (1,) * (len(extent) - dim - 1))

    loudness = one(*split[0])
    for cut in split[1:]:
        loudness = loudness * one(*cut)
    return loudness


def scatter_about(stream_key, dims, spread, reach, shards=(), kind=jnp.bfloat16):
    result = spread * jax.random.normal(stream_key, dims, jnp.float32)
    if shards:
        result = result * level_of(stream_key, dims, shards, -0.22, 0.18)
    return jnp.clip(result, -reach, reach).astype(kind)


def setup_inputs(seed: int = 0) -> dict:
    keys = jax.random.split(jax.random.key(seed), 13)
    query_input = scatter_about(keys[0], (TOKENS, D), 1.0, 6.0, ((0, 16),))
    query_cotangent = scatter_about(keys[1], (TOKENS, QKW), (TOKENS ** -0.5), 0.046875, ((0, 16), (1, 2)))
    branch_output = scatter_about(keys[2], (TOKENS, VW), 1.0, 6.0, ((0, 16),))
    layer_cotangent = scatter_about(keys[3], (TOKENS, D), (TOKENS ** -0.5), 0.046875, ((0, 16), (1, 2)))
    query_weight = scatter_about(keys[4], (D, QKW), D ** -0.5, 0.09375, ((0, 16), (1, 2)), jnp.float32)
    output_weight = scatter_about(keys[5], (VW, D), VW ** -0.5, 0.125, ((0, 16), (1, 2)), jnp.float32)
    query_basis = scatter_about(keys[6], (D, R), D ** -0.5, 0.09375, ((0, 16),))
    output_basis = scatter_about(keys[7], (VW, R), VW ** -0.5, 0.125, ((0, 16),))
    query_first = draw_query_first(jax.random.fold_in(keys[12], 71), 0)
    query_second = jnp.clip(jnp.exp(math.log(2.0) - 2.0794415 * jax.random.uniform(keys[9], (R, QKW), jnp.float32) ** level_of(keys[9], (R, QKW), ((0, 16), (1, 2)), -0.2, 0.2)), 0.25, 2.0)
    output_first = draw_output_first(jax.random.fold_in(keys[12], 71), 0)
    output_second = jnp.clip(jnp.exp(math.log(2.0) - 2.0794415 * jax.random.uniform(keys[11], (R, D), jnp.float32) ** level_of(keys[11], (R, D), ((0, 16), (1, 2)), -0.2, 0.2)), 0.25, 2.0)
    return dict(query_input=query_input, query_cotangent=query_cotangent, branch_output=branch_output, layer_cotangent=layer_cotangent, query_weight=query_weight, output_weight=output_weight, query_basis=query_basis, output_basis=output_basis, query_first=query_first, query_second=query_second, output_first=output_first, output_second=output_second)


beta_first = 0.6
beta_second = 0.8
step_rate = 0.01
small_eps = 1e-06

def project(inputs, basis, cotangent):
    inner = jnp.dot(inputs.astype(jnp.float32), basis.astype(jnp.float32), precision=lax.Precision.HIGHEST, preferred_element_type=jnp.float32)
    return jnp.dot(inner.T, cotangent.astype(jnp.float32), precision=lax.Precision.HIGHEST, preferred_element_type=jnp.float32)

def advance(first, second, projected, basis, weight):
    first_next = beta_first * first + (1.0 - beta_first) * projected
    second_next = beta_second * second + (1.0 - beta_second) * projected * projected
    normed = first_next / jnp.sqrt(second_next)
    scale = lax.rsqrt(jnp.mean(normed * normed) + small_eps)
    rounded = normed.astype(jnp.bfloat16)
    update = scale * jnp.dot(basis.astype(jnp.float32), rounded.astype(jnp.float32), precision=lax.Precision.HIGHEST, preferred_element_type=jnp.float32)
    copy = (weight - step_rate * update).astype(jnp.bfloat16)
    return (update, first_next, second_next, copy)

def reference(query_input, query_cotangent, branch_output, layer_cotangent, query_weight, output_weight, query_basis, output_basis, query_first, query_second, output_first, output_second):
    projected_q = project(query_input, query_basis, query_cotangent)
    projected_o = project(branch_output, output_basis, layer_cotangent)
    update_q, first_q, second_q, copy_q = advance(query_first, query_second, projected_q, query_basis, query_weight)
    update_o, first_o, second_o, copy_o = advance(output_first, output_second, projected_o, output_basis, output_weight)
    return (update_q, update_o, first_q, second_q, first_o, second_o, copy_q, copy_o)
```

```python
import functools

import jax
import jax.numpy as jnp
from jax import lax
from jax.experimental import pallas as pl
from jax.experimental.pallas import tpu as pltpu
from jax.sharding import PartitionSpec as P

MESH = pl.DeviceIdType.MESH
DMA = pltpu.SemaphoreType.DMA

beta_first = 0.6
beta_second = 0.8
step_rate = 0.01
small_eps = 1e-06


def here():
    return lax.axis_index("fs"), lax.axis_index("rep"), lax.axis_index("tp")


def flip(rep, bit):
    if bit == 1:
        return rep + 1 - 2 * lax.rem(rep, 2)
    return lax.rem(rep + 2, 4)


def remote(src, dst, send, recv, device):
    return pltpu.make_async_remote_copy(
        src_ref=src, dst_ref=dst, send_sem=send, recv_sem=recv, device_id=device, device_id_type=MESH
    )


def greet(devices):
    barrier = pltpu.get_barrier_semaphore()
    for device in devices:
        pl.semaphore_signal(barrier, inc=1, device_id=device, device_id_type=MESH)
    pl.semaphore_wait(barrier, len(devices))


class Line:
    def __init__(self, n, view, send, recv):
        self.n, self.view, self.send_sem, self.recv_sem = n, view, send, recv
        self.fs, self.rep, self.tp = here()
        self.done = 0

    def tick(self):
        if 0 < self.done < self.n:
            self.arrive(self.done)
        if self.done + 1 < self.n:
            self.start(self.done + 1)
        self.done += 1

    def outgoing(self, step, way):
        fs, n = self.fs, self.n
        if way == 0:
            block, peer = fs - step + 1, fs + 1
            present = jnp.logical_and(block >= 0, peer < n)
        else:
            block, peer = fs + step - 1, fs - 1
            present = jnp.logical_and(block < n, peer >= 0)
        block = lax.rem(block + n, n)
        peer = lax.rem(peer + n, n)
        view = self.view(block)
        sems = (self.send_sem.at[way, step - 1], self.recv_sem.at[way, step - 1])
        return remote(view, view, *sems, (peer, self.rep, self.tp)), present

    def incoming(self, step, way):
        fs, n = self.fs, self.n
        block = fs - step if way == 0 else fs + step
        present = block >= 0 if way == 0 else block < n
        block = lax.rem(block + n, n)
        view = self.view(block)
        sems = (self.send_sem.at[way, step - 1], self.recv_sem.at[way, step - 1])
        return remote(view, view, *sems, (fs, self.rep, self.tp)), present, block

    def start(self, step):
        for way in (0, 1):
            copy, present = self.outgoing(step, way)

            @pl.when(present)
            def _():
                copy.start()

    def arrive(self, step):
        for way in (0, 1):
            copy, present, _ = self.incoming(step, way)

            @pl.when(present)
            def _():
                copy.wait_recv()

    def sent(self):
        for step in range(1, self.n):
            for way in (0, 1):
                copy, present = self.outgoing(step, way)

                @pl.when(present)
                def _():
                    copy.wait_send()


def when(present, body):
    if present is True:
        body()
    else:
        pl.when(present)(body)


class Gather:
    bits = ((1, 2), (2, 1))

    def __init__(self, n, view, line_sems, one_sems, two_sems):
        self.n, self.view, self.one_sems, self.two_sems = n, view, one_sems, two_sems
        self.fs, self.rep, self.tp = here()
        self.line = Line(n, lambda b: view(self.rep * n + b, None), *line_sems)

    def slots(self, step):
        return [(0, 0)] if step == 0 else [(0, 2 * step - 1), (1, 2 * step)]

    def block_of(self, step, way):
        if step == 0:
            return self.fs, True
        block = self.fs - step if way == 0 else self.fs + step
        present = block >= 0 if way == 0 else block < self.n
        return lax.rem(block + self.n, self.n), present

    def one(self, block, slot, half):
        peer = flip(self.rep, self.bits[half][0])
        view = self.view(self.rep * self.n + block, half)
        return remote(view, view, *[s.at[half, slot] for s in self.one_sems], (self.fs, peer, self.tp))

    def one_in(self, block, slot, half):
        peer = flip(self.rep, self.bits[half][0])
        view = self.view(peer * self.n + block, half)
        return remote(view, view, *[s.at[half, slot] for s in self.one_sems], (self.fs, peer, self.tp))

    def two(self, block, slot, half, which):
        peer = flip(self.rep, self.bits[half][1])
        held = self.rep if which == 0 else flip(self.rep, self.bits[half][0])
        view = self.view(held * self.n + block, half)
        return remote(view, view, *[s.at[half, which, slot] for s in self.two_sems], (self.fs, peer, self.tp))

    def two_in(self, block, slot, half, which):
        peer = flip(self.rep, self.bits[half][1])
        held = peer if which == 0 else flip(peer, self.bits[half][0])
        view = self.view(held * self.n + block, half)
        return remote(view, view, *[s.at[half, which, slot] for s in self.two_sems], (self.fs, peer, self.tp))

    def each(self, step, action):
        for way, slot in self.slots(step):
            block, present = self.block_of(step, way)
            when(present, lambda: action(block, slot))

    def launch(self, step):
        def action(block, slot):
            for half in (0, 1):
                self.one(block, slot, half).start()
            for half in (0, 1):
                self.two(block, slot, half, 0).start()

        self.each(step, action)

    def start(self):
        self.line.start(1)
        self.launch(0)

    def arrive(self, step):
        self.line.arrive(step)
        if step < self.n - 1:
            self.line.start(step + 1)
        self.launch(step)

    def relay(self, step):
        def action(block, slot):
            for half in (0, 1):
                self.one_in(block, slot, half).wait_recv()
                self.two(block, slot, half, 1).start()

        self.each(step, action)

    def finish(self, step):
        def action(block, slot):
            for half in (0, 1):
                for which in (0, 1):
                    self.two_in(block, slot, half, which).wait_recv()

        self.each(step, action)

    def drain(self):
        def action(block, slot):
            for half in (0, 1):
                self.one(block, slot, half).wait_send()
                for which in (0, 1):
                    self.two(block, slot, half, which).wait_send()

        for step in range(self.n):
            self.each(step, action)
        self.line.sent()


class Scatter:
    def __init__(self, n, part, one, mid, two, total, out, late, one_sems, two_sems, line_sems):
        self.n, self.part, self.heard, self.mid_ref, self.two = n, part, one, mid, two
        self.total, self.out, self.late = total, out, late
        self.one_sems, self.two_sems, self.line_sems = one_sems, two_sems, line_sems
        self.fs, self.rep, self.tp = here()
        self.chunks, _, group, self.width = part.shape
        self.rows = group // n

    def peers(self, c):
        first, second = ((1, 2), (2, 1))[c % 2]
        return flip(self.rep, first), flip(self.rep, second), second

    def first(self, c, slot):
        near, _, second = self.peers(c)
        group = near if slot == 0 else flip(near, second)
        sems = [s.at[c, slot] for s in self.one_sems]
        return remote(self.part.at[c, group], self.heard.at[c, slot], *sems, (self.fs, near, self.tp))

    def second(self, c):
        _, far, _ = self.peers(c)
        sems = [s.at[c] for s in self.two_sems]
        return remote(self.mid_ref.at[c], self.two.at[c], *sems, (self.fs, far, self.tp))

    def third(self, c, j):
        f = lax.rem(self.fs + j, self.n)
        sems = [s.at[c, j - 1] for s in self.line_sems]
        return remote(self.out.at[c, j - 1], self.late.at[c, j - 1], *sems, (f, self.rep, self.tp))

    def compute(self, c, inner, cotangent):
        tile = min(256, self.width)
        rank = inner.shape[0] * inner.shape[1]

        def step(i, _):
            span = pl.ds(pl.multiple_of(c * self.width + i * tile, tile), tile)
            value = jnp.dot(
                inner[...].reshape(rank, -1), cotangent[:, span], preferred_element_type=jnp.float32
            )
            here_span = pl.ds(pl.multiple_of(i * tile, tile), tile)
            self.part[c, :, :, here_span] = value.astype(jnp.bfloat16).reshape(4, -1, tile)
            return 0

        lax.fori_loop(0, self.width // tile, step, 0)

    def send(self, c):
        for slot in (1, 0):
            self.first(c, slot).start()

    def middle(self, c):
        f32 = jnp.float32
        _, far, _ = self.peers(c)
        self.first(c, 1).wait_recv()
        value = self.part[c, far].astype(f32) + self.heard[c, 1].astype(f32)
        self.mid_ref[c] = value.astype(jnp.bfloat16)
        self.second(c).start()
        self.first(c, 0).wait_recv()
        self.total[c] = self.part[c, self.rep].astype(f32) + self.heard[c, 0].astype(f32)

    def rows_of(self, c, f):
        span = pl.ds(pl.multiple_of(f * self.rows, self.rows), self.rows)
        return self.total[c, span, :] + self.two[c, span, :].astype(jnp.float32)

    def cross(self, c):
        self.second(c).wait_recv()
        for j in range(1, self.n):
            value = self.rows_of(c, lax.rem(self.fs + j, self.n))
            self.out[c, j - 1] = value.astype(jnp.bfloat16)
            self.third(c, j).start()

    def final(self, c):
        value = self.rows_of(c, self.fs)
        for j in range(1, self.n):
            self.third(c, j).wait_recv()
            value = value + self.late[c, j - 1].astype(jnp.float32)
        return value

    def drain(self):
        for c in range(self.chunks):
            for slot in (0, 1):
                self.first(c, slot).wait_send()
            self.second(c).wait_send()
            for j in range(1, self.n):
                self.third(c, j).wait_send()


class Weights:
    def __init__(self, n, views, send, recv):
        self.lines = [Line(n, v, send.at[i], recv.at[i]) for i, v in enumerate(views)]
        self.n = n
        self.todo = [(step, line) for step in range(1, n) for line in self.lines]

    def tick(self, count):
        for _ in range(count):
            if self.todo:
                step, line = self.todo.pop(0)
                if step > 1:
                    line.arrive(step - 1)
                line.start(step)

    def finish(self):
        self.tick(len(self.todo))
        for line in self.lines:
            line.arrive(self.n - 1)

    def sent(self):
        for line in self.lines:
            line.sent()


def main_kernel(
    n,
    xq_hbm, cq_hbm, xo_hbm, co_hbm, wq_hbm, wo_hbm, bq_hbm, bo_hbm, fq_hbm, sq_hbm, fo_hbm, so_hbm,
    nq_ref, no_ref, gwq_ref, gwo_ref, hq_ref, ho_ref, nfq_ref, nsq_ref, nfo_ref, nso_ref, tot_ref,
    xq, cq, xo, co, wq, wo, fq, sq, fo, so, gbq, gbo, inq, ino,
    part_q, one_q, mid_q, two_q, total_q, out_q, late_q,
    part_o, one_o, mid_o, two_o, total_o, out_o, late_o,
    gs, local, *sems,
):
    fs, rep, tp = here()
    mine = rep * n + fs
    f32, b16 = jnp.float32, jnp.bfloat16
    sems = list(sems)

    def take():
        pair = (sems.pop(0), sems.pop(0))
        return pair

    half = bq_hbm.shape[1] // 2
    own = pl.ds(pl.multiple_of(tp * half, half), half)
    copies = [
        pltpu.make_async_copy(src, dst, local.at[i])
        for i, (src, dst) in enumerate(
            [
                (bo_hbm.at[:, own], gbo.at[mine]), (bq_hbm.at[:, own], gbq.at[mine]),
                (wq_hbm, wq), (wo_hbm, wo), (xo_hbm, xo), (co_hbm, co), (xq_hbm, xq), (cq_hbm, cq),
                (fo_hbm, fo), (so_hbm, so), (fq_hbm, fq), (sq_hbm, sq),
            ]
        )
    ]
    for copy in copies:
        copy.start()
    copies[0].wait()
    copies[1].wait()
    peers = [(lax.rem(fs + k, n), rep, tp) for k in range(1, n)]
    peers += [(fs, flip(rep, bit), tp) for bit in (1, 2)] + [(fs, rep, 1 - tp)]
    greet(peers)

    def rows_view(ref):
        rows = ref.shape[1] // 2

        def view(block, part):
            return ref.at[block] if part is None else ref.at[block, pl.ds(part * rows, rows)]

        return view

    def cols_view(ref):
        cols = ref.shape[2] // 2

        def view(block, part):
            return ref.at[block] if part is None else ref.at[block, :, pl.ds(part * cols, cols)]

        return view

    basis_o = Gather(n, rows_view(gbo), take(), take(), take())
    basis_q = Gather(n, rows_view(gbq), take(), take(), take())
    norm_o = Gather(n, cols_view(no_ref), take(), take(), take())
    norm_q = Gather(n, cols_view(nq_ref), take(), take(), take())
    norm_s = Gather(n, cols_view(gs), take(), take(), take())
    sum_o = Scatter(n, part_o, one_o, mid_o, two_o, total_o, out_o, late_o, take(), take(), take())
    sum_q = Scatter(n, part_q, one_q, mid_q, two_q, total_q, out_q, late_q, take(), take(), take())
    swap_s, swap_r = take()
    share_s, share_r = take()
    pair_s, pair_r = take()
    weight_s, weight_r = take()

    views = []
    for ref, pieces in ((gwq_ref, 2), (gwo_ref, 4)):
        rows = ref.shape[1] // pieces
        for p in range(pieces):
            views.append(lambda b, ref=ref, p=p, rows=rows: ref.at[b, pl.ds(p * rows, rows)])
    weights = Weights(n, views, weight_s, weight_r)

    basis_o.start()
    basis_q.start()
    copies[2].wait()
    copies[3].wait()
    gwq_ref[fs] = wq[...].astype(b16)
    gwo_ref[fs] = wo[...].astype(b16)

    for step in range(1, n):
        basis_o.arrive(step)
        basis_q.arrive(step)
        basis_o.relay(step - 1)
        basis_q.relay(step - 1)
    weights.tick(2)
    basis_o.relay(n - 1)
    weights.tick(1)
    for step in range(n):
        basis_o.finish(step)

    def share(a, f):
        gb, out = ((gbq, hq_ref), (gbo, ho_ref))[a]
        return remote(
            gb.at[rep * n + f], out.at[f, :, own], share_s.at[a, f], share_r.at[a, f], (fs, rep, 1 - tp)
        )

    def share_in(a, f):
        gb, out = ((gbq, hq_ref), (gbo, ho_ref))[a]
        other = pl.ds(pl.multiple_of((1 - tp) * half, half), half)
        return remote(
            gb.at[rep * n + f], out.at[f, :, other], share_s.at[a, f], share_r.at[a, f], (fs, rep, 1 - tp)
        )

    def keep(a):
        gb, out = ((gbq, hq_ref), (gbo, ho_ref))[a]
        for f in range(n):
            out[f, :, own] = gb[rep * n + f]

    def swap(a, core):
        ref = (inq, ino)[a]
        return remote(ref.at[core], ref.at[core], swap_s.at[a], swap_r.at[a], (fs, rep, 1 - tp))

    def project(a):
        x, gb, out = ((xq, gbq, inq), (xo, gbo, ino))[a]
        tile = min(512, x.shape[0])

        def step(t, _):
            span = pl.ds(pl.multiple_of(t * tile, tile), tile)
            value = jnp.dot(x[span, :], gb[...].reshape(-1, half), preferred_element_type=f32)
            out[tp, :, span] = value.T.astype(b16)
            return 0

        lax.fori_loop(0, x.shape[0] // tile, step, 0)
        swap(a, tp).start()

    def norm(a, c, scatter):
        first, second, first_out, second_out, n_out = (
            (fq, sq, nfq_ref, nsq_ref, nq_ref), (fo, so, nfo_ref, nso_ref, no_ref)
        )[a]
        span = pl.ds(c * scatter.width, scatter.width)
        p = scatter.final(c)
        first_next = beta_first * first[:, span] + (1.0 - beta_first) * p
        second_next = beta_second * second[:, span] + (1.0 - beta_second) * p * p
        normed = first_next / jnp.sqrt(second_next)
        first_out[:, span] = first_next
        second_out[:, span] = second_next
        n_out[mine, :, span] = normed.astype(b16)
        square = normed * normed
        rows, cols = square.shape
        square = sum(square[:, k : k + 128] for k in range(0, cols, 128))
        square = sum(square[k : k + 8] for k in range(0, rows, 8))
        slot = pl.ds(a * 128, 128)
        gs[mine, :, slot] = square if c == 0 else gs[mine, :, slot] + square

    copies[4].wait()
    project(1)
    basis_q.relay(n - 1)
    for f in range(n):
        share(1, f).start()
    weights.tick(1)
    copies[5].wait()
    swap(1, 1 - tp).wait_recv()
    for c in range(sum_o.chunks):
        sum_o.compute(c, ino, co)
        sum_o.send(c)
    keep(1)
    weights.tick(1)
    for step in range(n):
        basis_q.finish(step)
    copies[6].wait()
    project(0)
    for f in range(n):
        share(0, f).start()
    weights.tick(1)
    for c in range(2):
        sum_o.middle(c)
    copies[7].wait()
    swap(0, 1 - tp).wait_recv()
    for c in range(sum_q.chunks):
        sum_q.compute(c, inq, cq)
        sum_q.send(c)
    for c in range(2, sum_o.chunks):
        sum_o.middle(c)
    weights.tick(1)
    for copy in copies[8:]:
        copy.wait()
    for c in range(2):
        sum_o.cross(c)
    for c in range(sum_q.chunks):
        sum_q.middle(c)
    for c in range(2, sum_o.chunks):
        sum_o.cross(c)
    keep(0)
    weights.tick(1)
    for c in range(sum_o.chunks):
        norm(1, c, sum_o)
    norm_o.start()
    for c in range(sum_q.chunks):
        sum_q.cross(c)
    for c in range(sum_q.chunks):
        norm(0, c, sum_q)
    norm_q.start()
    norm_s.start()
    norms = (norm_o, norm_q, norm_s)
    for step in range(1, n):
        for g in norms:
            g.arrive(step)
        for g in norms:
            g.relay(step - 1)
    weights.tick(3)
    for g in norms:
        g.relay(n - 1)
    for step in range(n):
        for g in norms:
            g.finish(step)
    tot_ref[0] = sum(gs[b] for b in range(4 * n))
    pair = remote(tot_ref.at[0], tot_ref.at[1], pair_s.at[0], pair_r.at[0], (fs, rep, 1 - tp))
    pair.start()
    weights.finish()
    pair.wait()
    for a in (0, 1):
        swap(a, tp).wait_send()
        for f in range(n):
            share(a, f).wait_send()
            share_in(a, f).wait_recv()
    for g in (basis_o, basis_q, *norms, sum_o, sum_q):
        g.drain()
    weights.sent()


def pairs(*shapes):
    return [DMA(shape) for shape in shapes for _ in (0, 1)]


def advance(n, *args):
    xq, cq, xo, co, wq, wo, bq, bo, fq, sq, fo, so = args
    f32, b16 = jnp.float32, jnp.bfloat16
    shape, vmem = jax.ShapeDtypeStruct, pltpu.VMEM
    rank = bq.shape[1]
    half = rank // 2
    rows = fq.shape[0]
    width_q, width_o = cq.shape[1] // 2, co.shape[1] // 4

    def scatter(chunks, width):
        return [
            vmem((chunks, 4, n * rows, width), b16),
            vmem((chunks, 2, n * rows, width), b16),
            vmem((chunks, n * rows, width), b16),
            vmem((chunks, n * rows, width), b16),
            vmem((chunks, n * rows, width), f32),
            vmem((chunks, n - 1, rows, width), b16),
            vmem((chunks, n - 1, rows, width), b16),
        ]

    slots = 2 * n - 1
    gather = [(2, n - 1), (2, slots), (2, 2, slots)]
    reduce = lambda chunks: [(chunks, 2), (chunks,), (chunks, n - 1)]
    spec = pl.BlockSpec(memory_space=pltpu.VMEM)
    return pl.pallas_call(
        functools.partial(main_kernel, n),
        out_shape=(
            shape((4 * n, rows, cq.shape[1]), b16),
            shape((4 * n, rows, co.shape[1]), b16),
            shape((n, *wq.shape), b16),
            shape((n, *wo.shape), b16),
            shape((n, *bq.shape), b16),
            shape((n, *bo.shape), b16),
            *[shape(a.shape, f32) for a in (fq, sq, fo, so)],
            shape((2, 8, 256), f32),
        ),
        in_specs=[pl.BlockSpec(memory_space=pltpu.HBM)] * 12,
        out_specs=(spec,) * 11,
        scratch_shapes=[vmem(a.shape, a.dtype) for a in (xq, cq, xo, co, wq, wo, fq, sq, fo, so)]
        + [vmem((4 * n, bq.shape[0], half), b16), vmem((4 * n, bo.shape[0], half), b16)]
        + [vmem((2, half, xq.shape[0]), b16), vmem((2, half, xo.shape[0]), b16)]
        + scatter(2, width_q)
        + scatter(4, width_o)
        + [vmem((4 * n, 8, 256), f32), DMA((12,))]
        + pairs(*(gather * 5), *reduce(4), *reduce(2), (2,), (2, n), (1,), (6, 2, n - 1)),
        compiler_params=pltpu.CompilerParams(
            collective_id=0, has_side_effects=True, vmem_limit_bytes=40 * 2**20
        ),
        name="advance",
    )(*[pltpu.with_memory_space_constraint(a, pltpu.HBM) for a in args])


def last_kernel(
    n,
    hq, ho, nq, no, gwq, gwo, nfq, nsq, nfo, nso, tot,
    uq_out, uo_out, nfq_out, nsq_out, nfo_out, nso_out, cq_out, co_out,
    uq, uo, cq, co, sems,
):
    fs = lax.axis_index("fs")
    f32, b16 = jnp.float32, jnp.bfloat16
    copies = []

    def put(src, dst):
        copy = pltpu.make_async_copy(src, dst, sems.at[len(copies)])
        copy.start()
        copies.append(copy)

    for src, dst in ((nfq, nfq_out), (nsq, nsq_out), (nfo, nfo_out), (nso, nso_out)):
        put(src, dst)
    rank = nq.shape[0]
    for a, (rows_ref, normed, weights, u, c, u_hbm, c_hbm) in enumerate(
        ((hq, nq, gwq, uq, cq, uq_out, cq_out), (ho, no, gwo, uo, co, uo_out, co_out))
    ):
        columns = normed.shape[1]
        total = jnp.sum(tot[:, :, a * 128 : (a + 1) * 128], axis=0)
        total = jnp.sum(jnp.sum(total, axis=0, keepdims=True), axis=1, keepdims=True)
        scale = lax.rsqrt(total / (rank * 2 * columns) + small_eps)
        tile = min(256, columns)
        mine = u_hbm.shape[0]
        block = 2 * tile if columns % (2 * tile) == 0 else tile

        for k in range(0, columns, block):

            def step(i, _):
                span = pl.ds(pl.multiple_of(k + i * tile, tile), tile)
                value = scale * jnp.dot(rows_ref[...], normed[:, span], preferred_element_type=f32)
                u[:, span] = value
                c[:, span] = (weights[:, span].astype(f32) - step_rate * value).astype(b16)
                return 0

            lax.fori_loop(0, block // tile, step, 0)
            span = pl.ds(k, block)
            put(u.at[pl.ds(pl.multiple_of(fs * mine, mine), mine), span], u_hbm.at[:, span])
            put(c.at[:, span], c_hbm.at[:, span])
    for copy in copies:
        copy.wait()


def body(n, *args):
    xq, cq, xo, co, wq, wo, bq, bo, fq, sq, fo, so = args
    f32, b16 = jnp.float32, jnp.bfloat16
    rank = bq.shape[1]
    nq, no, gwq, gwo, hq, ho, nfq, nsq, nfo, nso, tot = advance(n, *args)
    shape, vmem = jax.ShapeDtypeStruct, pltpu.VMEM
    flat = lambda a: a.reshape(-1, a.shape[2])
    hq, ho, nq, no, gwq, gwo = [flat(a) for a in (hq, ho, nq, no, gwq, gwo)]
    outs = (
        shape(wq.shape, f32), shape(wo.shape, f32), shape(fq.shape, f32), shape(fq.shape, f32),
        shape(fo.shape, f32), shape(fo.shape, f32), shape(gwq.shape, b16), shape(gwo.shape, b16),
    )
    wide = lambda a: vmem(a.shape, f32)
    spec = pl.BlockSpec(memory_space=pltpu.VMEM)
    return pl.pallas_call(
        functools.partial(last_kernel, n),
        out_shape=outs,
        in_specs=[spec] * 11,
        out_specs=(pl.BlockSpec(memory_space=pl.ANY),) * 8,
        scratch_shapes=[wide(gwq), wide(gwo)]
        + [vmem(gwq.shape, b16), vmem(gwo.shape, b16), DMA((4 + 2 + 2 * (wo.shape[1] // 256),))],
        compiler_params=pltpu.CompilerParams(vmem_limit_bytes=20 * 2**20),
        name="update",
    )(hq, ho, nq, no, gwq, gwo, nfq, nsq, nfo, nso, tot)


def solution(mesh):
    in_specs = (
        P(("fs", "rep"), None),
        P(("fs", "rep"), "tp"),
        P(("fs", "rep"), None),
        P(("fs", "rep"), "tp"),
        P(("rep", "fs"), "tp"),
        P(("rep", "fs"), "tp"),
        P(("rep", "fs"), None),
        P(("rep", "fs"), None),
        P(("rep", "fs"), "tp"),
        P(("rep", "fs"), "tp"),
        P(("rep", "fs"), "tp"),
        P(("rep", "fs"), "tp"),
    )
    out_specs = (
        P(("rep", "fs"), "tp"),
        P(("rep", "fs"), "tp"),
        P(("rep", "fs"), "tp"),
        P(("rep", "fs"), "tp"),
        P(("rep", "fs"), "tp"),
        P(("rep", "fs"), "tp"),
        P("rep", "tp"),
        P("rep", "tp"),
    )
    n = mesh.shape["fs"]
    assert mesh.shape["rep"] == 4 and mesh.shape["tp"] == 2
    return jax.shard_map(functools.partial(body, n), mesh=mesh, in_specs=in_specs, out_specs=out_specs, check_vma=False)
```

```python
import functools

import jax
import jax.numpy as jnp
from jax import lax
from jax.experimental import pallas as pl
from jax.experimental.pallas import tpu as pltpu
from jax.sharding import PartitionSpec as P

MESH = pl.DeviceIdType.MESH
DMA = pltpu.SemaphoreType.DMA

beta_first = 0.6
beta_second = 0.8
step_rate = 0.01
small_eps = 1e-06


def here():
    return lax.axis_index("fs"), lax.axis_index("rep"), lax.axis_index("tp")


def flip(rep, bit):
    if bit == 1:
        return rep + 1 - 2 * lax.rem(rep, 2)
    return lax.rem(rep + 2, 4)


def remote(src, dst, send, recv, device):
    return pltpu.make_async_remote_copy(
        src_ref=src, dst_ref=dst, send_sem=send, recv_sem=recv, device_id=device, device_id_type=MESH
    )


def greet(devices):
    barrier = pltpu.get_barrier_semaphore()
    for device in devices:
        pl.semaphore_signal(barrier, inc=1, device_id=device, device_id_type=MESH)
    pl.semaphore_wait(barrier, len(devices))


def when(present, body):
    if present is True:
        body()
    else:
        pl.when(present)(body)


def await_sent(view, sem):
    remote(view, view, sem, sem, here()).wait_send()


def await_heard(view, sem):
    remote(view, view, sem, sem, here()).wait_recv()


class Line:
    def __init__(self, n, view, send, recv):
        self.n, self.view, self.send_sem, self.recv_sem = n, view, send, recv
        self.fs, self.rep, self.tp = here()

    def outgoing(self, step, way):
        fs, n = self.fs, self.n
        if way == 0:
            block, peer = fs - step + 1, fs + 1
            present = jnp.logical_and(block >= 0, peer < n)
        else:
            block, peer = fs + step - 1, fs - 1
            present = jnp.logical_and(block < n, peer >= 0)
        block = lax.rem(block + n, n)
        peer = lax.rem(peer + n, n)
        view = self.view(block)
        return remote(view, view, self.send_sem.at[way], self.recv_sem.at[block], (peer, self.rep, self.tp)), present

    def start(self, step):
        for way in (0, 1):
            copy, present = self.outgoing(step, way)
            when(present, copy.start)

    def arrive(self, step):
        for way in (0, 1):
            block = self.fs - step if way == 0 else self.fs + step
            present = block >= 0 if way == 0 else block < self.n
            block = lax.rem(block + self.n, self.n)
            when(present, lambda: await_heard(self.view(block), self.recv_sem.at[block]))

    def sent(self, many):
        for place in range(self.n):
            right = place + 1 if place < self.n - 1 else 0
            left = self.n - place if place > 0 else 0

            def body():
                for way, count in enumerate((right, left)):
                    if count:
                        await_sent(many(count), self.send_sem.at[way])

            pl.when(self.fs == place)(body)


class Gather:
    bits = ((1, 2), (2, 1))

    def __init__(self, n, view, many, send, line, one, two):
        self.n, self.view, self.many, self.send_sem = n, view, many, send
        self.line, self.one_sem, self.two_sem = line, one, two
        self.fs, self.rep, self.tp = here()

    def slots(self, step):
        if step == 0:
            return [(self.fs, True)]
        left, right = self.fs - step, self.fs + step
        rem = lambda block: lax.rem(block + self.n, self.n)
        return [(rem(left), left >= 0), (rem(right), right < self.n)]

    def each(self, step, action):
        for block, present in self.slots(step):
            when(present, lambda: action(block))

    def one(self, block, half):
        peer = flip(self.rep, self.bits[half][0])
        view = self.view(self.rep * self.n + block, half)
        return remote(view, view, self.send_sem, self.one_sem.at[half, block], (self.fs, peer, self.tp))

    def two(self, block, half, which):
        peer = flip(self.rep, self.bits[half][1])
        held = self.rep if which == 0 else flip(self.rep, self.bits[half][0])
        view = self.view(held * self.n + block, half)
        return remote(view, view, self.send_sem, self.two_sem, (self.fs, peer, self.tp))

    def launch(self, step):
        def action(block):
            for half in (0, 1):
                self.one(block, half).start()
            for half in (0, 1):
                self.two(block, half, 0).start()

        self.each(step, action)

    def start(self):
        own = self.view(self.rep * self.n + self.fs, None)
        for step in range(1, self.n):
            for peer, present in self.slots(step):
                copy = remote(own, own, self.send_sem, self.line.at[self.fs], (peer, self.rep, self.tp))
                when(present, copy.start)
        self.launch(0)

    def arrive(self, step):
        self.each(step, lambda block: await_heard(self.view(self.rep * self.n + block, None), self.line.at[block]))
        self.launch(step)

    def relay(self, step):
        def action(block):
            for half in (0, 1):
                peer = flip(self.rep, self.bits[half][0])
                await_heard(self.view(peer * self.n + block, half), self.one_sem.at[half, block])
                self.two(block, half, 1).start()

        self.each(step, action)

    def events(self):
        n = self.n
        todo = [(self.relay, 0)]
        for step in range(1, n):
            todo.append((self.arrive, step))
            if step >= 2:
                todo.append((self.relay, step - 1))
        return todo + ([(self.relay, n - 1)] if n > 1 else [])

    def finish(self):
        await_heard(self.many(2 * self.n), self.two_sem)

    def drain(self):
        await_sent(self.many(4 * self.n - 1), self.send_sem)


class Scatter:
    def __init__(self, n, part, one, mid, two, total, out, late, send, one_sem, two_sem, line_sem):
        self.n, self.part, self.heard, self.mid_ref, self.two = n, part, one, mid, two
        self.total, self.out, self.late = total, out, late
        self.send_sem, self.one_sem, self.two_sem, self.line_sem = send, one_sem, two_sem, line_sem
        self.fs, self.rep, self.tp = here()
        self.chunks, _, group, self.width = part.shape
        self.rows = group // n

    def peers(self, c):
        first, second = ((1, 2), (2, 1))[c % 2]
        return flip(self.rep, first), flip(self.rep, second), second

    def compute(self, c, inner, cotangent):
        tile = min(256, self.width)
        rank = inner.shape[0] * inner.shape[1]

        def step(i, _):
            span = pl.ds(pl.multiple_of(c * self.width + i * tile, tile), tile)
            value = jnp.dot(
                inner[...].reshape(rank, -1), cotangent[:, span], preferred_element_type=jnp.float32
            )
            here_span = pl.ds(pl.multiple_of(i * tile, tile), tile)
            self.part[c, :, :, here_span] = value.astype(jnp.bfloat16).reshape(4, -1, tile)
            return 0

        lax.fori_loop(0, self.width // tile, step, 0)

    def send(self, c):
        near, _, second = self.peers(c)
        for slot, group in ((1, flip(near, second)), (0, near)):
            remote(
                self.part.at[c, group], self.heard.at[c, slot], self.send_sem.at[0], self.one_sem.at[c],
                (self.fs, near, self.tp),
            ).start()

    def middle(self, c):
        f32 = jnp.float32
        _, far, _ = self.peers(c)
        await_heard(self.heard.at[c], self.one_sem.at[c])
        value = self.part[c, far].astype(f32) + self.heard[c, 1].astype(f32)
        self.mid_ref[c] = value.astype(jnp.bfloat16)
        remote(
            self.mid_ref.at[c], self.two.at[c], self.send_sem.at[1], self.two_sem.at[c], (self.fs, far, self.tp)
        ).start()
        self.total[c] = self.part[c, self.rep].astype(f32) + self.heard[c, 0].astype(f32)

    def rows_of(self, c, f):
        span = pl.ds(pl.multiple_of(f * self.rows, self.rows), self.rows)
        return self.total[c, span, :] + self.two[c, span, :].astype(jnp.float32)

    def cross(self, c):
        await_heard(self.two.at[c], self.two_sem.at[c])
        for j in range(1, self.n):
            f = lax.rem(self.fs + j, self.n)
            self.out[c, j - 1] = self.rows_of(c, f).astype(jnp.bfloat16)
            remote(
                self.out.at[c, j - 1], self.late.at[c, j - 1], self.send_sem.at[2], self.line_sem.at[c],
                (f, self.rep, self.tp),
            ).start()

    def final(self, c):
        value = self.rows_of(c, self.fs)
        await_heard(self.late.at[c], self.line_sem.at[c])
        for j in range(1, self.n):
            value = value + self.late[c, j - 1].astype(jnp.float32)
        return value

    def drain(self):
        await_sent(self.heard, self.send_sem.at[0])
        await_sent(self.mid_ref, self.send_sem.at[1])
        await_sent(self.out, self.send_sem.at[2])


class Weights:
    def __init__(self, n, views, many, send, recv):
        self.lines = [Line(n, v, send.at[i], recv.at[i]) for i, v in enumerate(views)]
        self.n, self.many = n, many
        self.todo = [(step, line) for step in range(1, n) for line in self.lines]

    def tick(self, count):
        for _ in range(count):
            if self.todo:
                step, line = self.todo.pop(0)
                if step > 1:
                    line.arrive(step - 1)
                line.start(step)

    def finish(self):
        self.tick(len(self.todo))
        for line in self.lines:
            line.arrive(self.n - 1)

    def sent(self):
        for line, many in zip(self.lines, self.many):
            line.sent(many)


def main_kernel(
    n,
    xq_hbm, cq_hbm, xo_hbm, co_hbm, wq_hbm, wo_hbm, bq_hbm, bo_hbm, fq_hbm, sq_hbm, fo_hbm, so_hbm,
    nq_ref, no_ref, gwq_ref, gwo_ref, hq_ref, ho_ref, nfq_ref, nsq_ref, nfo_ref, nso_ref, tot_ref,
    xq, cq, xo, co, wq, wo, fq, sq, fo, so, gbq, gbo, inq, ino,
    part_q, one_q, mid_q, two_q, total_q, out_q, late_q,
    part_o, one_o, mid_o, two_o, total_o, out_o, late_o,
    gs, local, *sems,
):
    fs, rep, tp = here()
    mine = rep * n + fs
    f32, b16 = jnp.float32, jnp.bfloat16
    sems = list(sems)
    take = lambda count: [sems.pop(0) for _ in range(count)]

    half = bq_hbm.shape[1] // 2
    own = pl.ds(pl.multiple_of(tp * half, half), half)
    copies = [
        pltpu.make_async_copy(src, dst, local.at[i])
        for i, (src, dst) in enumerate(
            [
                (bo_hbm.at[:, own], gbo.at[mine]), (bq_hbm.at[:, own], gbq.at[mine]),
                (wq_hbm, wq), (wo_hbm, wo), (xo_hbm, xo), (co_hbm, co), (xq_hbm, xq), (cq_hbm, cq),
                (fo_hbm, fo), (so_hbm, so), (fq_hbm, fq), (sq_hbm, sq),
            ]
        )
    ]
    for copy in copies:
        copy.start()
    copies[0].wait()
    copies[1].wait()
    peers = [(lax.rem(fs + k, n), rep, tp) for k in range(1, n)]
    peers += [(fs, flip(rep, bit), tp) for bit in (1, 2)] + [(fs, rep, 1 - tp)]
    greet(peers)

    def rows_view(ref):
        rows = ref.shape[1] // 2

        def view(block, part):
            return ref.at[block] if part is None else ref.at[block, pl.ds(part * rows, rows)]

        return view, lambda count: ref.at[pl.ds(0, count)]

    def cols_view(ref, index=0, count=1):
        cols = ref.shape[2] // (2 * count)

        def view(block, part):
            start, size = (0, 2 * cols) if part is None else (part * cols, cols)
            return ref.at[block, :, pl.ds(index * 2 * cols + start, size)]

        return view, lambda k: ref.at[pl.ds(0, k), :, pl.ds(index * 2 * cols, 2 * cols)]

    basis_o = Gather(n, *rows_view(gbo), *take(4))
    basis_q = Gather(n, *rows_view(gbq), *take(4))
    norm_o = [Gather(n, *cols_view(no_ref, i, 2), *take(4)) for i in range(2)]
    norm_q = Gather(n, *cols_view(nq_ref), *take(4))
    norm_s = Gather(n, *cols_view(gs), *take(4))
    sum_o = Scatter(n, part_o, one_o, mid_o, two_o, total_o, out_o, late_o, *take(4))
    sum_q = Scatter(n, part_q, one_q, mid_q, two_q, total_q, out_q, late_q, *take(4))
    swap_s, swap_r, share_s, share_r, pair_s, pair_r, weight_s, weight_r = take(8)

    views, many = [], []
    for ref, pieces in ((gwq_ref, 2), (gwo_ref, 4)):
        rows = ref.shape[1] // pieces
        for p in range(pieces):
            views.append(lambda b, ref=ref, p=p, rows=rows: ref.at[b, pl.ds(p * rows, rows)])
            many.append(lambda k, ref=ref, p=p, rows=rows: ref.at[pl.ds(0, k), pl.ds(p * rows, rows)])
    weights = Weights(n, views, many, weight_s, weight_r)

    basis_o.start()
    basis_q.start()
    copies[2].wait()
    copies[3].wait()
    gwq_ref[fs] = wq[...].astype(b16)
    gwo_ref[fs] = wo[...].astype(b16)

    queue = basis_q.events()

    def turn(count):
        for _ in range(count):
            if queue:
                action, step = queue.pop(0)
                action(step)

    for step in range(1, n):
        basis_o.arrive(step)
        basis_o.relay(step - 1)
        if step == 2:
            turn(1)
    basis_o.relay(n - 1)
    turn(2)
    basis_o.finish()

    def share(a):
        gb, out = ((gbq, hq_ref), (gbo, ho_ref))[a]
        for f in range(n):
            view = out.at[f, :, own]
            remote(gb.at[rep * n + f], view, share_s.at[a], share_r.at[a], (fs, rep, 1 - tp)).start()

    def shared(a):
        gb, out = ((gbq, hq_ref), (gbo, ho_ref))[a]
        other = pl.ds(pl.multiple_of((1 - tp) * half, half), half)
        await_heard(out.at[:, :, other], share_r.at[a])
        await_sent(gb.at[pl.ds(0, n)], share_s.at[a])

    def keep(a):
        gb, out = ((gbq, hq_ref), (gbo, ho_ref))[a]
        for f in range(n):
            out[f, :, own] = gb[rep * n + f]

    tokens = xq.shape[0]
    tile = min(512, tokens)

    def swap(a, t):
        ref = (inq, ino)[a]
        view = ref.at[tp, :, pl.ds(pl.multiple_of(t * tile, tile), tile)]
        return remote(view, view, swap_s.at[a], swap_r.at[a], (fs, rep, 1 - tp))

    def project(a):
        x, gb, out = ((xq, gbq, inq), (xo, gbo, ino))[a]

        def step(t, _):
            span = pl.ds(pl.multiple_of(t * tile, tile), tile)
            value = jnp.dot(x[span, :], gb[...].reshape(-1, half), preferred_element_type=f32)
            out[tp, :, span] = value.T.astype(b16)
            swap(a, t).start()
            return 0

        lax.fori_loop(0, tokens // tile, step, 0)

    def swapped(a):
        await_heard((inq, ino)[a].at[1 - tp], swap_r.at[a])

    def norm(a, c, scatter):
        first, second, first_out, second_out, n_out = (
            (fq, sq, nfq_ref, nsq_ref, nq_ref), (fo, so, nfo_ref, nso_ref, no_ref)
        )[a]
        span = pl.ds(c * scatter.width, scatter.width)
        p = scatter.final(c)
        first_next = beta_first * first[:, span] + (1.0 - beta_first) * p
        second_next = beta_second * second[:, span] + (1.0 - beta_second) * p * p
        normed = first_next / jnp.sqrt(second_next)
        first_out[:, span] = first_next
        second_out[:, span] = second_next
        n_out[mine, :, span] = normed.astype(b16)
        square = normed * normed
        rows, cols = square.shape
        square = sum(square[:, k : k + 128] for k in range(0, cols, 128))
        square = sum(square[k : k + 8] for k in range(0, rows, 8))
        slot = pl.ds(a * 128, 128)
        gs[mine, :, slot] = square if c == 0 else gs[mine, :, slot] + square

    copies[4].wait()
    project(1)
    turn(2)
    weights.tick(2)
    copies[5].wait()
    swapped(1)
    chunks = sum_o.chunks
    quarter = chunks // 4
    for c in range(chunks):
        sum_o.compute(c, ino, co)
        if c < 2 * quarter:
            sum_o.send(c)
        if c == 2 * quarter:
            turn(1)
            weights.tick(2)
    turn(len(queue))
    keep(1)
    weights.tick(2)

    def group(i):
        return range(i * quarter, (i + 1) * quarter)

    for c in group(0):
        sum_o.middle(c)
    for c in group(2):
        sum_o.send(c)
    for c in group(1):
        sum_o.middle(c)
    for c in group(3):
        sum_o.send(c)
    for c in group(0):
        sum_o.cross(c)
    for copy in copies[6:]:
        copy.wait()
    for c in group(2):
        sum_o.middle(c)
    for c in group(1):
        sum_o.cross(c)
    weights.tick(1)
    basis_q.finish()
    project(0)
    for c in group(3):
        sum_o.middle(c)
    for c in group(2):
        sum_o.cross(c)
    swapped(0)
    for c in range(sum_q.chunks):
        sum_q.compute(c, inq, cq)
        sum_q.send(c)
    for c in group(3):
        sum_o.cross(c)
    for i in (0, 1):
        for c in group(i):
            norm(1, c, sum_o)
    norm_o[0].start()
    for c in range(sum_q.chunks):
        sum_q.middle(c)
    for c in range(sum_q.chunks):
        sum_q.cross(c)
    for i in (2, 3):
        for c in group(i):
            norm(1, c, sum_o)
    norm_o[1].start()
    queue.extend(norm_o[0].events())
    turn(2)
    share(1)
    share(0)
    keep(0)
    for c in range(sum_q.chunks):
        norm(0, c, sum_q)
    norm_q.start()
    norm_s.start()
    weights.tick(3)
    later = [*zip(norm_o[1].events(), norm_q.events(), norm_s.events())]
    for k, steps in enumerate(later):
        turn(1)
        for action, step in steps:
            action(step)
        weights.tick(1)
    turn(len(queue))
    norms = (*norm_o, norm_q, norm_s)
    for g in norms:
        g.finish()
    tot_ref[0] = sum(gs[b] for b in range(4 * n))
    pair = remote(tot_ref.at[0], tot_ref.at[1], pair_s.at[0], pair_r.at[0], (fs, rep, 1 - tp))
    pair.start()
    weights.finish()
    pair.wait()
    for a in (0, 1):
        await_sent((inq, ino)[a].at[tp], swap_s.at[a])
        shared(a)
    for g in (basis_o, basis_q, *norms, sum_o, sum_q):
        g.drain()
    weights.sent()


def advance(n, *args):
    xq, cq, xo, co, wq, wo, bq, bo, fq, sq, fo, so = args
    f32, b16 = jnp.float32, jnp.bfloat16
    shape, vmem = jax.ShapeDtypeStruct, pltpu.VMEM
    rank = bq.shape[1]
    half = rank // 2
    rows = fq.shape[0]
    width_q, width_o = cq.shape[1] // 2, co.shape[1] // 8

    def scatter(chunks, width):
        return [
            vmem((chunks, 4, n * rows, width), b16),
            vmem((chunks, 2, n * rows, width), b16),
            vmem((chunks, n * rows, width), b16),
            vmem((chunks, n * rows, width), b16),
            vmem((chunks, n * rows, width), f32),
            vmem((chunks, n - 1, rows, width), b16),
            vmem((chunks, n - 1, rows, width), b16),
        ]

    gather = [(), (n,), (2, n), ()]
    reduce = lambda chunks: [(3,), (chunks,), (chunks,), (chunks,)]
    shapes = gather * 6 + reduce(8) + reduce(2) + [(2,), (2,), (2,), (2,), (1,), (1,), (6, 2), (6, n)]
    spec = pl.BlockSpec(memory_space=pltpu.VMEM)
    return pl.pallas_call(
        functools.partial(main_kernel, n),
        out_shape=(
            shape((4 * n, rows, cq.shape[1]), b16),
            shape((4 * n, rows, co.shape[1]), b16),
            shape((n, *wq.shape), b16),
            shape((n, *wo.shape), b16),
            shape((n, *bq.shape), b16),
            shape((n, *bo.shape), b16),
            *[shape(a.shape, f32) for a in (fq, sq, fo, so)],
            shape((2, 8, 256), f32),
        ),
        in_specs=[pl.BlockSpec(memory_space=pltpu.HBM)] * 12,
        out_specs=(spec,) * 11,
        scratch_shapes=[vmem(a.shape, a.dtype) for a in (xq, cq, xo, co, wq, wo, fq, sq, fo, so)]
        + [vmem((4 * n, bq.shape[0], half), b16), vmem((4 * n, bo.shape[0], half), b16)]
        + [vmem((2, half, xq.shape[0]), b16), vmem((2, half, xo.shape[0]), b16)]
        + scatter(2, width_q)
        + scatter(8, width_o)
        + [vmem((4 * n, 8, 256), f32), DMA((12,))]
        + [DMA(a) if a else DMA for a in shapes],
        compiler_params=pltpu.CompilerParams(
            collective_id=0, has_side_effects=True, vmem_limit_bytes=40 * 2**20
        ),
        name="advance",
    )(*[pltpu.with_memory_space_constraint(a, pltpu.HBM) for a in args])


def last_kernel(
    n,
    hq, ho, nq, no, gwq, gwo, nfq, nsq, nfo, nso, tot,
    uq_out, uo_out, nfq_out, nsq_out, nfo_out, nso_out, cq_out, co_out,
    uq, uo, cq, co, sems,
):
    fs = lax.axis_index("fs")
    f32, b16 = jnp.float32, jnp.bfloat16
    copies = []

    def put(src, dst):
        copy = pltpu.make_async_copy(src, dst, sems.at[len(copies)])
        copy.start()
        copies.append(copy)

    for src, dst in ((nfq, nfq_out), (nsq, nsq_out), (nfo, nfo_out), (nso, nso_out)):
        put(src, dst)
    rank = nq.shape[0]
    for a, (rows_ref, normed, weights, u, c, u_hbm, c_hbm) in enumerate(
        ((hq, nq, gwq, uq, cq, uq_out, cq_out), (ho, no, gwo, uo, co, uo_out, co_out))
    ):
        columns = normed.shape[1]
        total = jnp.sum(tot[:, :, a * 128 : (a + 1) * 128], axis=0)
        total = jnp.sum(jnp.sum(total, axis=0, keepdims=True), axis=1, keepdims=True)
        scale = lax.rsqrt(total / (rank * 2 * columns) + small_eps)
        tile = min(256, columns)
        mine = u_hbm.shape[0]
        block = 2 * tile if columns % (2 * tile) == 0 else tile

        for k in range(0, columns, block):

            def step(i, _):
                span = pl.ds(pl.multiple_of(k + i * tile, tile), tile)
                value = scale * jnp.dot(rows_ref[...], normed[:, span], preferred_element_type=f32)
                u[:, span] = value
                c[:, span] = (weights[:, span].astype(f32) - step_rate * value).astype(b16)
                return 0

            lax.fori_loop(0, block // tile, step, 0)
            span = pl.ds(k, block)
            put(u.at[pl.ds(pl.multiple_of(fs * mine, mine), mine), span], u_hbm.at[:, span])
            put(c.at[:, span], c_hbm.at[:, span])
    for copy in copies:
        copy.wait()


def body(n, *args):
    xq, cq, xo, co, wq, wo, bq, bo, fq, sq, fo, so = args
    f32, b16 = jnp.float32, jnp.bfloat16
    rank = bq.shape[1]
    nq, no, gwq, gwo, hq, ho, nfq, nsq, nfo, nso, tot = advance(n, *args)
    shape, vmem = jax.ShapeDtypeStruct, pltpu.VMEM
    flat = lambda a: a.reshape(-1, a.shape[2])
    hq, ho, nq, no, gwq, gwo = [flat(a) for a in (hq, ho, nq, no, gwq, gwo)]
    outs = (
        shape(wq.shape, f32), shape(wo.shape, f32), shape(fq.shape, f32), shape(fq.shape, f32),
        shape(fo.shape, f32), shape(fo.shape, f32), shape(gwq.shape, b16), shape(gwo.shape, b16),
    )
    wide = lambda a: vmem(a.shape, f32)
    spec = pl.BlockSpec(memory_space=pltpu.VMEM)
    return pl.pallas_call(
        functools.partial(last_kernel, n),
        out_shape=outs,
        in_specs=[spec] * 11,
        out_specs=(pl.BlockSpec(memory_space=pl.ANY),) * 8,
        scratch_shapes=[wide(gwq), wide(gwo)]
        + [vmem(gwq.shape, b16), vmem(gwo.shape, b16), DMA((4 + 2 + 2 * (wo.shape[1] // 256),))],
        compiler_params=pltpu.CompilerParams(vmem_limit_bytes=20 * 2**20),
        name="update",
    )(hq, ho, nq, no, gwq, gwo, nfq, nsq, nfo, nso, tot)


def solution(mesh):
    in_specs = (
        P(("fs", "rep"), None),
        P(("fs", "rep"), "tp"),
        P(("fs", "rep"), None),
        P(("fs", "rep"), "tp"),
        P(("rep", "fs"), "tp"),
        P(("rep", "fs"), "tp"),
        P(("rep", "fs"), None),
        P(("rep", "fs"), None),
        P(("rep", "fs"), "tp"),
        P(("rep", "fs"), "tp"),
        P(("rep", "fs"), "tp"),
        P(("rep", "fs"), "tp"),
    )
    out_specs = (
        P(("rep", "fs"), "tp"),
        P(("rep", "fs"), "tp"),
        P(("rep", "fs"), "tp"),
        P(("rep", "fs"), "tp"),
        P(("rep", "fs"), "tp"),
        P(("rep", "fs"), "tp"),
        P("rep", "tp"),
        P("rep", "tp"),
    )
    n = mesh.shape["fs"]
    assert mesh.shape["rep"] == 4 and mesh.shape["tp"] == 2
    return jax.shard_map(functools.partial(body, n), mesh=mesh, in_specs=in_specs, out_specs=out_specs, check_vma=False)
```

```python
import functools

import jax
import jax.numpy as jnp
from jax import lax
from jax.experimental import pallas as pl
from jax.experimental.pallas import tpu as pltpu
from jax.sharding import PartitionSpec as P

MESH = pl.DeviceIdType.MESH
DMA = pltpu.SemaphoreType.DMA

beta_first = 0.6
beta_second = 0.8
step_rate = 0.01
small_eps = 1e-06


def here():
    return lax.axis_index("fs"), lax.axis_index("rep"), lax.axis_index("tp")


def flip(rep, bit):
    if bit == 1:
        return rep + 1 - 2 * lax.rem(rep, 2)
    return lax.rem(rep + 2, 4)


def remote(src, dst, send, recv, device):
    return pltpu.make_async_remote_copy(
        src_ref=src, dst_ref=dst, send_sem=send, recv_sem=recv, device_id=device, device_id_type=MESH
    )


def greet(devices):
    barrier = pltpu.get_barrier_semaphore()
    for device in devices:
        pl.semaphore_signal(barrier, inc=1, device_id=device, device_id_type=MESH)
    pl.semaphore_wait(barrier, len(devices))


def when(present, body):
    if present is True:
        body()
    else:
        pl.when(present)(body)


def await_sent(view, sem):
    remote(view, view, sem, sem, here()).wait_send()


def await_heard(view, sem):
    remote(view, view, sem, sem, here()).wait_recv()


class Line:
    def __init__(self, n, view, send, recv):
        self.n, self.view, self.send_sem, self.recv_sem = n, view, send, recv
        self.fs, self.rep, self.tp = here()

    def outgoing(self, step, way):
        fs, n = self.fs, self.n
        if way == 0:
            block, peer = fs - step + 1, fs + 1
            present = jnp.logical_and(block >= 0, peer < n)
        else:
            block, peer = fs + step - 1, fs - 1
            present = jnp.logical_and(block < n, peer >= 0)
        block = lax.rem(block + n, n)
        peer = lax.rem(peer + n, n)
        view = self.view(block)
        return remote(view, view, self.send_sem.at[way], self.recv_sem.at[block], (peer, self.rep, self.tp)), present

    def start(self, step):
        for way in (0, 1):
            copy, present = self.outgoing(step, way)
            when(present, copy.start)

    def arrive(self, step):
        for way in (0, 1):
            block = self.fs - step if way == 0 else self.fs + step
            present = block >= 0 if way == 0 else block < self.n
            block = lax.rem(block + self.n, self.n)
            when(present, lambda: await_heard(self.view(block), self.recv_sem.at[block]))

    def sent(self, many):
        for place in range(self.n):
            right = place + 1 if place < self.n - 1 else 0
            left = self.n - place if place > 0 else 0

            def body():
                for way, count in enumerate((right, left)):
                    if count:
                        await_sent(many(count), self.send_sem.at[way])

            pl.when(self.fs == place)(body)


class Gather:
    bits = ((1, 2), (2, 1))

    def __init__(self, n, view, many, send, line, one, two):
        self.n, self.view, self.many, self.send_sem = n, view, many, send
        self.line, self.one_sem, self.two_sem = line, one, two
        self.fs, self.rep, self.tp = here()

    def slots(self, step):
        if step == 0:
            return [(self.fs, True)]
        left, right = self.fs - step, self.fs + step
        rem = lambda block: lax.rem(block + self.n, self.n)
        return [(rem(left), left >= 0), (rem(right), right < self.n)]

    def each(self, step, action):
        for block, present in self.slots(step):
            when(present, lambda: action(block))

    def one(self, block, half):
        peer = flip(self.rep, self.bits[half][0])
        view = self.view(self.rep * self.n + block, half)
        return remote(view, view, self.send_sem, self.one_sem.at[half, block], (self.fs, peer, self.tp))

    def two(self, block, half, which):
        peer = flip(self.rep, self.bits[half][1])
        held = self.rep if which == 0 else flip(self.rep, self.bits[half][0])
        view = self.view(held * self.n + block, half)
        return remote(view, view, self.send_sem, self.two_sem, (self.fs, peer, self.tp))

    def launch(self, step):
        def action(block):
            for half in (0, 1):
                self.one(block, half).start()
            for half in (0, 1):
                self.two(block, half, 0).start()

        self.each(step, action)

    def start(self):
        own = self.view(self.rep * self.n + self.fs, None)
        for step in range(1, self.n):
            for peer, present in self.slots(step):
                copy = remote(own, own, self.send_sem, self.line.at[self.fs], (peer, self.rep, self.tp))
                when(present, copy.start)
        self.launch(0)

    def arrive(self, step):
        self.each(step, lambda block: await_heard(self.view(self.rep * self.n + block, None), self.line.at[block]))
        self.launch(step)

    def relay(self, step):
        def action(block):
            for half in (0, 1):
                peer = flip(self.rep, self.bits[half][0])
                await_heard(self.view(peer * self.n + block, half), self.one_sem.at[half, block])
                self.two(block, half, 1).start()

        self.each(step, action)

    def events(self):
        n = self.n
        todo = [(self.relay, 0)]
        for step in range(1, n):
            todo.append((self.arrive, step))
            if step >= 2:
                todo.append((self.relay, step - 1))
        return todo + ([(self.relay, n - 1)] if n > 1 else [])

    def finish(self):
        await_heard(self.many(2 * self.n), self.two_sem)

    def drain(self):
        await_sent(self.many(4 * self.n - 1), self.send_sem)


class Scatter:
    def __init__(self, n, part, one, mid, two, total, out, late, send, one_sem, two_sem, line_sem):
        self.n, self.part, self.heard, self.mid_ref, self.two = n, part, one, mid, two
        self.total, self.out, self.late = total, out, late
        self.send_sem, self.one_sem, self.two_sem, self.line_sem = send, one_sem, two_sem, line_sem
        self.fs, self.rep, self.tp = here()
        self.chunks, _, group, self.width = part.shape
        self.rows = group // n

    def peers(self, c):
        first, second = ((1, 2), (2, 1))[c % 2]
        return flip(self.rep, first), flip(self.rep, second), second

    def compute(self, c, inner, cotangent):
        tile = min(256, self.width)
        rank = inner.shape[0] * inner.shape[1]

        def step(i, _):
            span = pl.ds(pl.multiple_of(c * self.width + i * tile, tile), tile)
            value = jnp.dot(
                inner[...].reshape(rank, -1), cotangent[:, span], preferred_element_type=jnp.float32
            )
            here_span = pl.ds(pl.multiple_of(i * tile, tile), tile)
            self.part[c, :, :, here_span] = value.astype(jnp.bfloat16).reshape(4, -1, tile)
            return 0

        lax.fori_loop(0, self.width // tile, step, 0)

    def send(self, c):
        near, _, second = self.peers(c)
        for slot, group in ((1, flip(near, second)), (0, near)):
            remote(
                self.part.at[c, group], self.heard.at[c, slot], self.send_sem.at[0], self.one_sem.at[c],
                (self.fs, near, self.tp),
            ).start()

    def middle(self, c):
        f32 = jnp.float32
        _, far, _ = self.peers(c)
        await_heard(self.heard.at[c], self.one_sem.at[c])
        value = self.part[c, far].astype(f32) + self.heard[c, 1].astype(f32)
        self.mid_ref[c] = value.astype(jnp.bfloat16)
        remote(
            self.mid_ref.at[c], self.two.at[c], self.send_sem.at[1], self.two_sem.at[c], (self.fs, far, self.tp)
        ).start()
        self.total[c] = self.part[c, self.rep].astype(f32) + self.heard[c, 0].astype(f32)

    def sums(self, c, rows):
        return self.total[c, rows, :] + self.two[c, rows, :].astype(jnp.float32)

    def stream(self, c, place, way, heard):
        n, r = self.n, self.rows
        rows = pl.ds((place + 1) * r, (n - 1 - place) * r) if way == 0 else pl.ds(0, place * r)
        value = self.sums(c, rows)
        if heard:
            value = value + self.late[c, way, rows, :].astype(jnp.float32)
        self.out[c, rows, :] = value.astype(jnp.bfloat16)
        peer = (place + 1 if way == 0 else place - 1, self.rep, self.tp)
        remote(
            self.out.at[c, rows], self.late.at[c, way, rows], self.send_sem.at[2 + way],
            self.line_sem.at[c, way], peer,
        ).start()

    def hear(self, c, place, way):
        n, r = self.n, self.rows
        rows = pl.ds(place * r, (n - place) * r) if way == 0 else pl.ds(0, (place + 1) * r)
        await_heard(self.late.at[c, way, rows], self.line_sem.at[c, way])

    def cross(self, c):
        await_heard(self.two.at[c], self.two_sem.at[c])
        for place, way in ((0, 0), (self.n - 1, 1)):
            pl.when(self.fs == place)(lambda: self.stream(c, place, way, False))

    def onward(self, c, turn):
        for place in range(1, self.n - 1):
            way = turn if 2 * place < self.n else 1 - turn

            def body():
                self.hear(c, place, way)
                self.stream(c, place, way, True)

            pl.when(self.fs == place)(body)

    def final(self, c):
        n, r = self.n, self.rows
        for place, way in ((0, 1), (n - 1, 0)):
            pl.when(self.fs == place)(lambda: self.hear(c, place, way))
        own = pl.ds(pl.multiple_of(self.fs * r, r), r)
        self.total[c, own, :] = self.sums(c, own)
        for way, present in ((0, self.fs > 0), (1, self.fs < n - 1)):

            def body():
                self.total[c, own, :] = self.total[c, own, :] + self.late[c, way, own, :].astype(jnp.float32)

            pl.when(present)(body)
        return self.total[c, own, :]

    def drain(self):
        await_sent(self.heard, self.send_sem.at[0])
        await_sent(self.mid_ref, self.send_sem.at[1])
        n, r = self.n, self.rows
        for place in range(n):

            def body():
                for way, count in ((0, n - 1 - place), (1, place)):
                    if count:
                        await_sent(self.out.at[:, pl.ds(0, count * r)], self.send_sem.at[2 + way])

            pl.when(self.fs == place)(body)


class Weights:
    def __init__(self, n, views, many, send, recv):
        self.lines = [Line(n, v, send.at[i], recv.at[i]) for i, v in enumerate(views)]
        self.n, self.many = n, many
        self.todo = [(step, line) for step in range(1, n) for line in self.lines]

    def tick(self, count):
        for _ in range(count):
            if self.todo:
                step, line = self.todo.pop(0)
                if step > 1:
                    line.arrive(step - 1)
                line.start(step)

    def finish(self):
        self.tick(len(self.todo))
        for line in self.lines:
            line.arrive(self.n - 1)

    def sent(self):
        for line, many in zip(self.lines, self.many):
            line.sent(many)


def pieces_of(*refs):
    return [min(most, ref.shape[-2] // 8) for most, ref in zip((4, 8), refs)]


def main_kernel(
    n,
    xq_hbm, cq_hbm, xo_hbm, co_hbm, wq_hbm, wo_hbm, bq_hbm, bo_hbm, fq_hbm, sq_hbm, fo_hbm, so_hbm,
    nq_ref, no_ref, gwq_ref, gwo_ref, hq_ref, ho_ref, nfq_ref, nsq_ref, nfo_ref, nso_ref, tot_ref,
    xq, cq, xo, co, wq, wo, fq, sq, fo, so, gbq, gbo, inq, ino,
    part_q, one_q, mid_q, two_q, total_q, out_q, late_q,
    part_o, one_o, mid_o, two_o, total_o, out_o, late_o,
    gs, local, *sems,
):
    fs, rep, tp = here()
    mine = rep * n + fs
    f32, b16 = jnp.float32, jnp.bfloat16
    sems = list(sems)
    take = lambda count: [sems.pop(0) for _ in range(count)]

    half = bq_hbm.shape[1] // 2
    own = pl.ds(pl.multiple_of(tp * half, half), half)
    copies = [
        pltpu.make_async_copy(src, dst, local.at[i])
        for i, (src, dst) in enumerate(
            [
                (bo_hbm.at[:, own], gbo.at[mine]), (bq_hbm.at[:, own], gbq.at[mine]),
                (wq_hbm, wq), (wo_hbm, wo), (xo_hbm, xo), (co_hbm, co), (xq_hbm, xq), (cq_hbm, cq),
                (fo_hbm, fo), (so_hbm, so), (fq_hbm, fq), (sq_hbm, sq),
            ]
        )
    ]
    for copy in copies:
        copy.start()
    copies[0].wait()
    copies[1].wait()
    peers = [(lax.rem(fs + k, n), rep, tp) for k in range(1, n)]
    peers += [(fs, flip(rep, bit), tp) for bit in (1, 2)] + [(fs, rep, 1 - tp)]
    greet(peers)

    def rows_view(ref):
        rows = ref.shape[1] // 2

        def view(block, part):
            return ref.at[block] if part is None else ref.at[block, pl.ds(part * rows, rows)]

        return view, lambda count: ref.at[pl.ds(0, count)]

    def cols_view(ref, index=0, count=1):
        cols = ref.shape[2] // (2 * count)

        def view(block, part):
            start, size = (0, 2 * cols) if part is None else (part * cols, cols)
            return ref.at[block, :, pl.ds(index * 2 * cols + start, size)]

        return view, lambda k: ref.at[pl.ds(0, k), :, pl.ds(index * 2 * cols, 2 * cols)]

    basis_o = Gather(n, *rows_view(gbo), *take(4))
    basis_q = Gather(n, *rows_view(gbq), *take(4))
    norm_o = [Gather(n, *cols_view(no_ref, i, 2), *take(4)) for i in range(2)]
    norm_q = Gather(n, *cols_view(nq_ref), *take(4))
    norm_s = Gather(n, *cols_view(gs), *take(4))
    sum_o = Scatter(n, part_o, one_o, mid_o, two_o, total_o, out_o, late_o, *take(4))
    sum_q = Scatter(n, part_q, one_q, mid_q, two_q, total_q, out_q, late_q, *take(4))
    swap_s, swap_r, share_s, share_r, pair_s, pair_r, weight_s, weight_r = take(8)

    views, many = [], []
    for ref, pieces in zip((gwq_ref, gwo_ref), pieces_of(gwq_ref, gwo_ref)):
        rows = ref.shape[1] // pieces
        for p in range(pieces):
            views.append(lambda b, ref=ref, p=p, rows=rows: ref.at[b, pl.ds(p * rows, rows)])
            many.append(lambda k, ref=ref, p=p, rows=rows: ref.at[pl.ds(0, k), pl.ds(p * rows, rows)])
    weights = Weights(n, views, many, weight_s, weight_r)

    basis_o.start()
    basis_q.start()
    copies[2].wait()
    copies[3].wait()
    gwq_ref[fs] = wq[...].astype(b16)
    gwo_ref[fs] = wo[...].astype(b16)

    queue = basis_q.events()

    def turn(count):
        for _ in range(count):
            if queue:
                action, step = queue.pop(0)
                action(step)

    for step in range(1, n):
        basis_o.arrive(step)
        basis_o.relay(step - 1)
        if step == 2:
            turn(1)
    basis_o.relay(n - 1)
    turn(1)
    basis_o.finish()

    def share(a):
        gb, out = ((gbq, hq_ref), (gbo, ho_ref))[a]
        for f in range(n):
            view = out.at[f, :, own]
            remote(gb.at[rep * n + f], view, share_s.at[a], share_r.at[a], (fs, rep, 1 - tp)).start()

    def shared(a):
        gb, out = ((gbq, hq_ref), (gbo, ho_ref))[a]
        other = pl.ds(pl.multiple_of((1 - tp) * half, half), half)
        await_heard(out.at[:, :, other], share_r.at[a])
        await_sent(gb.at[pl.ds(0, n)], share_s.at[a])

    def keep(a):
        gb, out = ((gbq, hq_ref), (gbo, ho_ref))[a]
        for f in range(n):
            out[f, :, own] = gb[rep * n + f]

    tokens = xq.shape[0]
    tile = min(512, tokens)

    def swap(a, t):
        ref = (inq, ino)[a]
        view = ref.at[tp, :, pl.ds(pl.multiple_of(t * tile, tile), tile)]
        return remote(view, view, swap_s.at[a], swap_r.at[a], (fs, rep, 1 - tp))

    def project(a):
        x, gb, out = ((xq, gbq, inq), (xo, gbo, ino))[a]

        def step(t, _):
            span = pl.ds(pl.multiple_of(t * tile, tile), tile)
            value = jnp.dot(x[span, :], gb[...].reshape(-1, half), preferred_element_type=f32)
            out[tp, :, span] = value.T.astype(b16)
            swap(a, t).start()
            return 0

        lax.fori_loop(0, tokens // tile, step, 0)

    def swapped(a):
        await_heard((inq, ino)[a].at[1 - tp], swap_r.at[a])

    def norm(a, c, scatter):
        first, second, first_out, second_out, n_out = (
            (fq, sq, nfq_ref, nsq_ref, nq_ref), (fo, so, nfo_ref, nso_ref, no_ref)
        )[a]
        span = pl.ds(c * scatter.width, scatter.width)
        p = scatter.final(c)
        first_next = beta_first * first[:, span] + (1.0 - beta_first) * p
        second_next = beta_second * second[:, span] + (1.0 - beta_second) * p * p
        normed = first_next / jnp.sqrt(second_next)
        first_out[:, span] = first_next
        second_out[:, span] = second_next
        n_out[mine, :, span] = normed.astype(b16)
        square = normed * normed
        rows, cols = square.shape
        square = sum(square[:, k : k + 128] for k in range(0, cols, 128))
        square = sum(square[k : k + 8] for k in range(0, rows, 8))
        slot = pl.ds(a * 128, 128)
        gs[mine, :, slot] = square if c == 0 else gs[mine, :, slot] + square

    copies[4].wait()
    project(1)
    turn(3)
    weights.tick(6)
    copies[5].wait()
    swapped(1)
    chunks = sum_o.chunks
    quarter = chunks // 4
    for c in range(chunks):
        sum_o.compute(c, ino, co)
        if c < 2 * quarter:
            sum_o.send(c)
        if c == 2 * quarter:
            turn(1)
            weights.tick(4)
    turn(len(queue))
    keep(1)
    weights.tick(4)

    def group(i):
        return range(i * quarter, (i + 1) * quarter)

    for c in group(0):
        sum_o.middle(c)
    for c in group(2):
        sum_o.send(c)
    for c in group(1):
        sum_o.middle(c)
    for c in group(3):
        sum_o.send(c)
    weights.tick(2)
    for copy in copies[6:]:
        copy.wait()
    basis_q.finish()
    project(0)
    for c in group(0):
        sum_o.cross(c)
    for c in group(2):
        sum_o.middle(c)
    swapped(0)
    for c in range(sum_q.chunks):
        sum_q.compute(c, inq, cq)
        sum_q.send(c)
    def cross(i):
        for c in group(i):
            sum_o.cross(c)

    def onward(i, turn):
        for c in group(i):
            sum_o.onward(c, turn)

    def both(i):
        for k in (i, i + 1):
            for c in group(k):
                norm(1, c, sum_o)

    cross(1)
    onward(0, 0)
    weights.tick(1)
    for c in group(3):
        sum_o.middle(c)
    cross(2)
    onward(1, 0)
    onward(0, 1)
    weights.tick(1)
    cross(3)
    onward(2, 0)
    onward(1, 1)
    weights.tick(1)
    for c in range(sum_q.chunks):
        sum_q.middle(c)
    onward(3, 0)
    onward(2, 1)
    weights.tick(1)
    for c in range(sum_q.chunks):
        sum_q.cross(c)
    both(0)
    norm_o[0].start()
    queue.extend(norm_o[0].events())
    onward(3, 1)
    for c in range(sum_q.chunks):
        sum_q.onward(c, 0)
    both(2)
    norm_o[1].start()
    weights.tick(2)
    for c in range(sum_q.chunks):
        sum_q.onward(c, 1)
    turn(2)
    weights.tick(2)
    for c in range(sum_q.chunks):
        norm(0, c, sum_q)
    norm_q.start()
    norm_s.start()
    weights.tick(4)
    turn(1)
    share(1)
    share(0)
    keep(0)
    turn(len(queue))
    later = [*zip(norm_o[1].events(), norm_q.events(), norm_s.events())]
    for k, steps in enumerate(later):
        for action, step in steps:
            action(step)
        weights.tick(2)
    norms = (*norm_o, norm_q, norm_s)
    for g in norms:
        g.finish()
    tot_ref[0] = sum(gs[b] for b in range(4 * n))
    pair = remote(tot_ref.at[0], tot_ref.at[1], pair_s.at[0], pair_r.at[0], (fs, rep, 1 - tp))
    pair.start()
    weights.finish()
    pair.wait()
    for a in (0, 1):
        await_sent((inq, ino)[a].at[tp], swap_s.at[a])
        shared(a)
    for g in (basis_o, basis_q, *norms, sum_o, sum_q):
        g.drain()
    weights.sent()


def advance(n, *args):
    xq, cq, xo, co, wq, wo, bq, bo, fq, sq, fo, so = args
    f32, b16 = jnp.float32, jnp.bfloat16
    shape, vmem = jax.ShapeDtypeStruct, pltpu.VMEM
    rank = bq.shape[1]
    half = rank // 2
    rows = fq.shape[0]
    width_q, width_o = cq.shape[1] // 2, co.shape[1] // 8

    def scatter(chunks, width):
        return [
            vmem((chunks, 4, n * rows, width), b16),
            vmem((chunks, 2, n * rows, width), b16),
            vmem((chunks, n * rows, width), b16),
            vmem((chunks, n * rows, width), b16),
            vmem((chunks, n * rows, width), f32),
            vmem((chunks, n * rows, width), b16),
            vmem((chunks, 2, n * rows, width), b16),
        ]

    pieces = sum(pieces_of(wq, wo))
    gather = [(), (n,), (2, n), ()]
    reduce = lambda chunks: [(4,), (chunks,), (chunks,), (chunks, 2)]
    shapes = gather * 6 + reduce(8) + reduce(2) + [(2,), (2,), (2,), (2,), (1,), (1,), (pieces, 2), (pieces, n)]
    spec = pl.BlockSpec(memory_space=pltpu.VMEM)
    return pl.pallas_call(
        functools.partial(main_kernel, n),
        out_shape=(
            shape((4 * n, rows, cq.shape[1]), b16),
            shape((4 * n, rows, co.shape[1]), b16),
            shape((n, *wq.shape), b16),
            shape((n, *wo.shape), b16),
            shape((n, *bq.shape), b16),
            shape((n, *bo.shape), b16),
            *[shape(a.shape, f32) for a in (fq, sq, fo, so)],
            shape((2, 8, 256), f32),
        ),
        in_specs=[pl.BlockSpec(memory_space=pltpu.HBM)] * 12,
        out_specs=(spec,) * 11,
        scratch_shapes=[vmem(a.shape, a.dtype) for a in (xq, cq, xo, co, wq, wo, fq, sq, fo, so)]
        + [vmem((4 * n, bq.shape[0], half), b16), vmem((4 * n, bo.shape[0], half), b16)]
        + [vmem((2, half, xq.shape[0]), b16), vmem((2, half, xo.shape[0]), b16)]
        + scatter(2, width_q)
        + scatter(8, width_o)
        + [vmem((4 * n, 8, 256), f32), DMA((12,))]
        + [DMA(a) if a else DMA for a in shapes],
        compiler_params=pltpu.CompilerParams(
            collective_id=0, has_side_effects=True, vmem_limit_bytes=40 * 2**20
        ),
        name="advance",
    )(*[pltpu.with_memory_space_constraint(a, pltpu.HBM) for a in args])


def last_kernel(
    n,
    hq, ho, nq, no, gwq, gwo, nfq, nsq, nfo, nso, tot,
    uq_out, uo_out, nfq_out, nsq_out, nfo_out, nso_out, cq_out, co_out,
    uq, uo, cq, co, sems,
):
    fs = lax.axis_index("fs")
    f32, b16 = jnp.float32, jnp.bfloat16
    copies = []

    def put(src, dst):
        copy = pltpu.make_async_copy(src, dst, sems.at[len(copies)])
        copy.start()
        copies.append(copy)

    for src, dst in ((nfq, nfq_out), (nsq, nsq_out), (nfo, nfo_out), (nso, nso_out)):
        put(src, dst)
    rank = nq.shape[0]
    for a, (rows_ref, normed, weights, u, c, u_hbm, c_hbm) in enumerate(
        ((hq, nq, gwq, uq, cq, uq_out, cq_out), (ho, no, gwo, uo, co, uo_out, co_out))
    ):
        columns = normed.shape[1]
        total = jnp.sum(tot[:, :, a * 128 : (a + 1) * 128], axis=0)
        total = jnp.sum(jnp.sum(total, axis=0, keepdims=True), axis=1, keepdims=True)
        scale = lax.rsqrt(total / (rank * 2 * columns) + small_eps)
        tile = min(256, columns)
        mine = u_hbm.shape[0]
        block = 2 * tile if columns % (2 * tile) == 0 else tile

        for k in range(0, columns, block):

            def step(i, _):
                span = pl.ds(pl.multiple_of(k + i * tile, tile), tile)
                value = scale * jnp.dot(rows_ref[...], normed[:, span], preferred_element_type=f32)
                u[:, span] = value
                c[:, span] = (weights[:, span].astype(f32) - step_rate * value).astype(b16)
                return 0

            lax.fori_loop(0, block // tile, step, 0)
            span = pl.ds(k, block)
            put(u.at[pl.ds(pl.multiple_of(fs * mine, mine), mine), span], u_hbm.at[:, span])
            put(c.at[:, span], c_hbm.at[:, span])
    for copy in copies:
        copy.wait()


def body(n, *args):
    xq, cq, xo, co, wq, wo, bq, bo, fq, sq, fo, so = args
    f32, b16 = jnp.float32, jnp.bfloat16
    rank = bq.shape[1]
    nq, no, gwq, gwo, hq, ho, nfq, nsq, nfo, nso, tot = advance(n, *args)
    shape, vmem = jax.ShapeDtypeStruct, pltpu.VMEM
    flat = lambda a: a.reshape(-1, a.shape[2])
    hq, ho, nq, no, gwq, gwo = [flat(a) for a in (hq, ho, nq, no, gwq, gwo)]
    outs = (
        shape(wq.shape, f32), shape(wo.shape, f32), shape(fq.shape, f32), shape(fq.shape, f32),
        shape(fo.shape, f32), shape(fo.shape, f32), shape(gwq.shape, b16), shape(gwo.shape, b16),
    )
    wide = lambda a: vmem(a.shape, f32)
    spec = pl.BlockSpec(memory_space=pltpu.VMEM)
    return pl.pallas_call(
        functools.partial(last_kernel, n),
        out_shape=outs,
        in_specs=[spec] * 11,
        out_specs=(pl.BlockSpec(memory_space=pl.ANY),) * 8,
        scratch_shapes=[wide(gwq), wide(gwo)]
        + [vmem(gwq.shape, b16), vmem(gwo.shape, b16), DMA((4 + 2 + 2 * (wo.shape[1] // 256),))],
        compiler_params=pltpu.CompilerParams(vmem_limit_bytes=20 * 2**20),
        name="update",
    )(hq, ho, nq, no, gwq, gwo, nfq, nsq, nfo, nso, tot)


def solution(mesh):
    in_specs = (
        P(("fs", "rep"), None),
        P(("fs", "rep"), "tp"),
        P(("fs", "rep"), None),
        P(("fs", "rep"), "tp"),
        P(("rep", "fs"), "tp"),
        P(("rep", "fs"), "tp"),
        P(("rep", "fs"), None),
        P(("rep", "fs"), None),
        P(("rep", "fs"), "tp"),
        P(("rep", "fs"), "tp"),
        P(("rep", "fs"), "tp"),
        P(("rep", "fs"), "tp"),
    )
    out_specs = (
        P(("rep", "fs"), "tp"),
        P(("rep", "fs"), "tp"),
        P(("rep", "fs"), "tp"),
        P(("rep", "fs"), "tp"),
        P(("rep", "fs"), "tp"),
        P(("rep", "fs"), "tp"),
        P("rep", "tp"),
        P("rep", "tp"),
    )
    n = mesh.shape["fs"]
    assert mesh.shape["rep"] == 4 and mesh.shape["tp"] == 2
    return jax.shard_map(functools.partial(body, n), mesh=mesh, in_specs=in_specs, out_specs=out_specs, check_vma=False)
```

```python
import functools

import jax
import jax.numpy as jnp
from jax import lax
from jax.experimental import pallas as pl
from jax.experimental.pallas import tpu as pltpu
from jax.sharding import PartitionSpec as P

MESH = pl.DeviceIdType.MESH
DMA = pltpu.SemaphoreType.DMA

beta_first = 0.6
beta_second = 0.8
step_rate = 0.01
small_eps = 1e-06


def here():
    return lax.axis_index("fs"), lax.axis_index("rep"), lax.axis_index("tp")


def flip(rep, bit):
    if bit == 1:
        return rep + 1 - 2 * lax.rem(rep, 2)
    return lax.rem(rep + 2, 4)


def remote(src, dst, send, recv, device):
    return pltpu.make_async_remote_copy(
        src_ref=src, dst_ref=dst, send_sem=send, recv_sem=recv, device_id=device, device_id_type=MESH
    )


def greet(devices):
    barrier = pltpu.get_barrier_semaphore()
    for device in devices:
        pl.semaphore_signal(barrier, inc=1, device_id=device, device_id_type=MESH)
    pl.semaphore_wait(barrier, len(devices))


def when(present, body):
    if present is True:
        body()
    else:
        pl.when(present)(body)


def await_sent(view, sem):
    remote(view, view, sem, sem, here()).wait_send()


def await_heard(view, sem):
    remote(view, view, sem, sem, here()).wait_recv()


class Line:
    def __init__(self, n, view, send, recv):
        self.n, self.view, self.send_sem, self.recv_sem = n, view, send, recv
        self.fs, self.rep, self.tp = here()

    def outgoing(self, step, way):
        fs, n = self.fs, self.n
        if way == 0:
            block, peer = fs - step + 1, fs + 1
            present = jnp.logical_and(block >= 0, peer < n)
        else:
            block, peer = fs + step - 1, fs - 1
            present = jnp.logical_and(block < n, peer >= 0)
        block = lax.rem(block + n, n)
        peer = lax.rem(peer + n, n)
        view = self.view(block)
        return remote(view, view, self.send_sem.at[way], self.recv_sem.at[block], (peer, self.rep, self.tp)), present

    def start(self, step, part=None):
        for way in (0, 1):
            copy, present = self.outgoing(step, way)
            if part is not None:
                right = 2 * self.fs >= self.n if (way == 0) == (part == 0) else 2 * self.fs < self.n
                present = jnp.logical_and(present, right)
            when(present, copy.start)

    def arrive(self, step):
        for way in (0, 1):
            block = self.fs - step if way == 0 else self.fs + step
            present = block >= 0 if way == 0 else block < self.n
            block = lax.rem(block + self.n, self.n)
            when(present, lambda: await_heard(self.view(block), self.recv_sem.at[block]))

    def sent(self, many):
        for place in range(self.n):
            right = place + 1 if place < self.n - 1 else 0
            left = self.n - place if place > 0 else 0

            def body():
                for way, count in enumerate((right, left)):
                    if count:
                        await_sent(many(count), self.send_sem.at[way])

            pl.when(self.fs == place)(body)


class Gather:
    bits = ((1, 2), (2, 1))

    def __init__(self, n, far, view, many, send, line, one, two):
        self.far = far and n > 3
        self.n, self.view, self.many, self.send_sem = n, view, many, send
        self.line, self.one_sem, self.two_sem = line, one, two
        self.fs, self.rep, self.tp = here()

    def slots(self, step):
        if step == 0:
            return [(self.fs, True)]
        left, right = self.fs - step, self.fs + step
        rem = lambda block: lax.rem(block + self.n, self.n)
        return [(rem(left), left >= 0), (rem(right), right < self.n)]

    def each(self, step, action):
        for block, present in self.slots(step):
            when(present, lambda: action(block))

    def one(self, block, half):
        peer = flip(self.rep, self.bits[half][0])
        view = self.view(self.rep * self.n + block, half)
        return remote(view, view, self.send_sem, self.one_sem.at[half, block], (self.fs, peer, self.tp))

    def two(self, block, half, which):
        peer = flip(self.rep, self.bits[half][1])
        held = self.rep if which == 0 else flip(self.rep, self.bits[half][0])
        view = self.view(held * self.n + block, half)
        return remote(view, view, self.send_sem, self.two_sem, (self.fs, peer, self.tp))

    def launch(self, step):
        def action(block):
            for half in (0, 1):
                self.one(block, half).start()
            for half in (0, 1):
                self.two(block, half, 0).start()

        self.each(step, action)

    def start(self):
        for step in range(1, self.n - 1 if self.far else self.n):
            for peer, present in self.slots(step):
                when(present, lambda: self.along(self.fs, peer))
        self.launch(0)

    def along(self, block, peer):
        view = self.view(self.rep * self.n + block, None)
        remote(view, view, self.send_sem, self.line.at[block], (peer, self.rep, self.tp)).start()

    def arrive(self, step):
        self.each(step, lambda block: await_heard(self.view(self.rep * self.n + block, None), self.line.at[block]))
        if self.far and step == self.n - 2:
            for place, block, peer in ((1, self.n - 1, 0), (self.n - 2, 0, self.n - 1)):
                pl.when(self.fs == place)(lambda: self.along(block, peer))
        self.launch(step)

    def relay(self, step):
        def action(block):
            for half in (0, 1):
                peer = flip(self.rep, self.bits[half][0])
                await_heard(self.view(peer * self.n + block, half), self.one_sem.at[half, block])
                self.two(block, half, 1).start()

        self.each(step, action)

    def events(self):
        n = self.n
        todo = [(self.relay, 0)]
        for step in range(1, n):
            todo.append((self.arrive, step))
            if step >= 2:
                todo.append((self.relay, step - 1))
        return todo + ([(self.relay, n - 1)] if n > 1 else [])

    def head(self):
        return [(self.relay, 0)] + [(self.arrive, step) for step in range(1, self.n - 1)]

    def rest(self):
        n = self.n
        return [(self.relay, 1), (self.arrive, n - 1)] + [(self.relay, step) for step in range(2, n)]

    def finish(self):
        await_heard(self.many(2 * self.n), self.two_sem)

    def drain(self):
        n = self.n
        for place in range(n):
            count = 4 * n - 1
            if self.far:
                count += -1 if place in (0, n - 1) else 1 if place in (1, n - 2) else 0
            pl.when(self.fs == place)(lambda: await_sent(self.many(count), self.send_sem))


class Scatter:
    def __init__(self, n, direct, part, one, mid, two, total, out, late, send, one_sem, two_sem, line_sem):
        self.n, self.part, self.heard, self.mid_ref, self.two = n, part, one, mid, two
        self.total, self.out, self.late = total, out, late
        self.send_sem, self.one_sem, self.two_sem, self.line_sem = send, one_sem, two_sem, line_sem
        self.fs, self.rep, self.tp = here()
        self.chunks, _, group, self.width = part.shape
        self.rows = group // n
        self.direct = direct

    def peers(self, c):
        first, second = ((1, 2), (2, 1))[c % 2]
        return flip(self.rep, first), flip(self.rep, second), second

    def compute(self, c, inner, cotangent):
        tile = min(256, self.width)
        rank = inner.shape[0] * inner.shape[1]

        def step(i, _):
            span = pl.ds(pl.multiple_of(c * self.width + i * tile, tile), tile)
            value = jnp.dot(
                inner[...].reshape(rank, -1), cotangent[:, span], preferred_element_type=jnp.float32
            )
            here_span = pl.ds(pl.multiple_of(i * tile, tile), tile)
            self.part[c, :, :, here_span] = value.astype(jnp.bfloat16).reshape(4, -1, tile)
            return 0

        lax.fori_loop(0, self.width // tile, step, 0)

    def send(self, c):
        near, _, second = self.peers(c)
        for slot, group in ((1, flip(near, second)), (0, near)):
            remote(
                self.part.at[c, group], self.heard.at[c, slot], self.send_sem.at[0], self.one_sem.at[c],
                (self.fs, near, self.tp),
            ).start()

    def middle(self, c):
        f32 = jnp.float32
        _, far, _ = self.peers(c)
        await_heard(self.heard.at[c], self.one_sem.at[c])
        value = self.part[c, far].astype(f32) + self.heard[c, 1].astype(f32)
        self.mid_ref[c] = value.astype(jnp.bfloat16)
        remote(
            self.mid_ref.at[c], self.two.at[c], self.send_sem.at[1], self.two_sem.at[c], (self.fs, far, self.tp)
        ).start()
        self.total[c] = self.part[c, self.rep].astype(f32) + self.heard[c, 0].astype(f32)

    def sums(self, c, rows):
        return self.total[c, rows, :] + self.two[c, rows, :].astype(jnp.float32)

    def stream(self, c, place, way, heard):
        n, r = self.n, self.rows
        rows = pl.ds((place + 1) * r, (n - 1 - place) * r) if way == 0 else pl.ds(0, place * r)
        value = self.sums(c, rows)
        if heard:
            value = value + self.late[c, way, rows, :].astype(jnp.float32)
        self.out[c, rows, :] = value.astype(jnp.bfloat16)
        peer = (place + 1 if way == 0 else place - 1, self.rep, self.tp)
        remote(
            self.out.at[c, rows], self.late.at[c, way, rows], self.send_sem.at[2 + way],
            self.line_sem.at[c, way], peer,
        ).start()

    def hear(self, c, place, way):
        n, r = self.n, self.rows
        rows = pl.ds(place * r, (n - place) * r) if way == 0 else pl.ds(0, (place + 1) * r)
        await_heard(self.late.at[c, way, rows], self.line_sem.at[c, way])

    def cross(self, c):
        await_heard(self.two.at[c], self.two_sem.at[c])
        if c >= self.direct:
            r = self.rows
            mine = pl.ds(pl.multiple_of(self.fs * r, r), r)
            for j in range(1, self.n):
                f = lax.rem(self.fs + j, self.n)
                rows = pl.ds(pl.multiple_of(f * r, r), r)
                self.out[c, rows, :] = self.sums(c, rows).astype(jnp.bfloat16)
                remote(
                    self.out.at[c, rows], self.late.at[c, 0, mine], self.send_sem.at[4],
                    self.line_sem.at[c, 0], (f, self.rep, self.tp),
                ).start()
            return
        for place, way in ((0, 0), (self.n - 1, 1)):
            pl.when(self.fs == place)(lambda: self.stream(c, place, way, False))

    def onward(self, c, turn):
        for place in range(1, self.n - 1):
            way = turn if 2 * place < self.n else 1 - turn

            def body():
                self.hear(c, place, way)
                self.stream(c, place, way, True)

            pl.when(self.fs == place)(body)

    def final(self, c):
        n, r = self.n, self.rows
        own = pl.ds(pl.multiple_of(self.fs * r, r), r)
        if c >= self.direct:
            value = self.sums(c, own)
            await_heard(self.late.at[c, 0, pl.ds(0, (n - 1) * r)], self.line_sem.at[c, 0])
            for j in range(1, n):
                f = lax.rem(self.fs + j, n)
                value = value + self.late[c, 0, pl.ds(pl.multiple_of(f * r, r), r), :].astype(jnp.float32)
            return value
        for place, way in ((0, 1), (n - 1, 0)):
            pl.when(self.fs == place)(lambda: self.hear(c, place, way))
        self.total[c, own, :] = self.sums(c, own)
        for way, present in ((0, self.fs > 0), (1, self.fs < n - 1)):

            def body():
                self.total[c, own, :] = self.total[c, own, :] + self.late[c, way, own, :].astype(jnp.float32)

            pl.when(present)(body)
        return self.total[c, own, :]

    def drain(self):
        await_sent(self.heard, self.send_sem.at[0])
        await_sent(self.mid_ref, self.send_sem.at[1])
        n, r = self.n, self.rows
        if self.direct < self.chunks:
            direct = pl.ds(self.direct, self.chunks - self.direct)
            await_sent(self.out.at[direct, pl.ds(0, (n - 1) * r)], self.send_sem.at[4])
        if self.direct == 0:
            return
        for place in range(n):

            def body():
                for way, count in ((0, n - 1 - place), (1, place)):
                    if count:
                        rows = pl.ds(0, count * r)
                        await_sent(self.out.at[pl.ds(0, self.direct), rows], self.send_sem.at[2 + way])

            pl.when(self.fs == place)(body)


class Weights:
    def __init__(self, n, views, many, send, recv):
        self.lines = [Line(n, v, send.at[i], recv.at[i]) for i, v in enumerate(views)]
        self.n, self.many = n, many
        self.todo = [(step, line, None) for step in range(1, n) for line in self.lines]

    def early(self, count):
        for k in range(count):
            step, line, _ = self.todo[k]
            line.start(step, 0)
            self.todo[k] = (step, line, 1)

    def tick(self, count):
        for _ in range(count):
            if self.todo:
                step, line, part = self.todo.pop(0)
                if step > 1:
                    line.arrive(step - 1)
                line.start(step, part)

    def finish(self):
        self.tick(len(self.todo))
        for line in self.lines:
            line.arrive(self.n - 1)

    def sent(self):
        for line, many in zip(self.lines, self.many):
            line.sent(many)


def pieces_of(*refs):
    return [min(most, ref.shape[-2] // 8) for most, ref in zip((4, 8), refs)]


def main_kernel(
    n,
    xq_hbm, cq_hbm, xo_hbm, co_hbm, wq_hbm, wo_hbm, bq_hbm, bo_hbm, fq_hbm, sq_hbm, fo_hbm, so_hbm,
    uq_ref, uo_ref, gwq_ref, gwo_ref, nfq_ref, nsq_ref, nfo_ref, nso_ref, tot_ref,
    xq, cq, xo, co, wq, wo, fq, sq, fo, so, gbq, gbo, inq, ino,
    part_q, one_q, mid_q, two_q, total_q, out_q, late_q,
    part_o, one_o, mid_o, two_o, total_o, out_o, late_o,
    nq_ref, no_ref, hq_ref, ho_ref, local, *sems,
):
    fs, rep, tp = here()
    mine = rep * n + fs
    f32, b16 = jnp.float32, jnp.bfloat16
    sems = list(sems)
    take = lambda count: [sems.pop(0) for _ in range(count)]

    half = bq_hbm.shape[1] // 2
    own = pl.ds(pl.multiple_of(tp * half, half), half)
    copies = [
        pltpu.make_async_copy(src, dst, local.at[i])
        for i, (src, dst) in enumerate(
            [
                (bo_hbm.at[:, own], gbo.at[mine]), (bq_hbm.at[:, own], gbq.at[mine]),
                (wq_hbm, wq), (wo_hbm, wo), (xo_hbm, xo), (co_hbm, co), (xq_hbm, xq), (cq_hbm, cq),
                (fo_hbm, fo), (so_hbm, so), (fq_hbm, fq), (sq_hbm, sq),
            ]
        )
    ]
    for copy in copies:
        copy.start()
    copies[0].wait()
    copies[1].wait()
    peers = [(lax.rem(fs + k, n), rep, tp) for k in range(1, n)]
    peers += [(fs, flip(rep, bit), tp) for bit in (1, 2)] + [(fs, rep, 1 - tp)]
    greet(peers)

    def rows_view(ref):
        rows = ref.shape[1] // 2

        def view(block, part):
            return ref.at[block] if part is None else ref.at[block, pl.ds(part * rows, rows)]

        return view, lambda count: ref.at[pl.ds(0, count)]

    def cols_view(ref, index=0, count=1):
        cols = ref.shape[2] // (2 * count)

        def view(block, part):
            start, size = (0, 2 * cols) if part is None else (part * cols, cols)
            return ref.at[block, :, pl.ds(index * 2 * cols + start, size)]

        return view, lambda k: ref.at[pl.ds(0, k), :, pl.ds(index * 2 * cols, 2 * cols)]

    basis_o = Gather(n, False, *rows_view(gbo), *take(4))
    basis_q = Gather(n, False, *rows_view(gbq), *take(4))
    norm_o = [Gather(n, True, *cols_view(no_ref, i, 2), *take(4)) for i in range(2)]
    norm_q = Gather(n, True, *cols_view(nq_ref), *take(4))
    sum_o = Scatter(n, 3 * part_o.shape[0] // 4, part_o, one_o, mid_o, two_o, total_o, out_o, late_o, *take(4))
    sum_q = Scatter(n, 0, part_q, one_q, mid_q, two_q, total_q, out_q, late_q, *take(4))
    swap_s, swap_r, share_s, share_r, pair_s, pair_r, weight_s, weight_r = take(8)

    views, many = [], []
    for ref, pieces in zip((gwq_ref, gwo_ref), pieces_of(gwq_ref, gwo_ref)):
        rows = ref.shape[1] // pieces
        for p in range(pieces):
            views.append(lambda b, ref=ref, p=p, rows=rows: ref.at[b, pl.ds(p * rows, rows)])
            many.append(lambda k, ref=ref, p=p, rows=rows: ref.at[pl.ds(0, k), pl.ds(p * rows, rows)])
    weights = Weights(n, views, many, weight_s, weight_r)

    basis_o.start()
    basis_q.start()
    copies[2].wait()
    copies[3].wait()
    gwq_ref[fs] = wq[...].astype(b16)
    gwo_ref[fs] = wo[...].astype(b16)
    weights.early(4)

    queue = basis_q.events()

    def turn(count):
        for _ in range(count):
            if queue:
                action, step = queue.pop(0)
                action(step)

    for step in range(1, n):
        basis_o.arrive(step)
        basis_o.relay(step - 1)
        if step == 2:
            turn(1)
    basis_o.relay(n - 1)
    turn(1)
    basis_o.finish()

    def share(a):
        gb, out = ((gbq, hq_ref), (gbo, ho_ref))[a]
        for f in range(n):
            view = out.at[f, :, own]
            remote(gb.at[rep * n + f], view, share_s.at[a], share_r.at[a], (fs, rep, 1 - tp)).start()

    def shared(a):
        gb, out = ((gbq, hq_ref), (gbo, ho_ref))[a]
        other = pl.ds(pl.multiple_of((1 - tp) * half, half), half)
        await_heard(out.at[:, :, other], share_r.at[a])
        await_sent(gb.at[pl.ds(0, n)], share_s.at[a])

    def keep(a):
        gb, out = ((gbq, hq_ref), (gbo, ho_ref))[a]
        for f in range(n):
            out[f, :, own] = gb[rep * n + f]

    tokens = xq.shape[0]
    tile = min(512, tokens)

    def swap(a, t):
        ref = (inq, ino)[a]
        view = ref.at[tp, :, pl.ds(pl.multiple_of(t * tile, tile), tile)]
        return remote(view, view, swap_s.at[a], swap_r.at[a], (fs, rep, 1 - tp))

    def project(a):
        x, gb, out = ((xq, gbq, inq), (xo, gbo, ino))[a]

        def step(t, _):
            span = pl.ds(pl.multiple_of(t * tile, tile), tile)
            value = jnp.dot(x[span, :], gb[...].reshape(-1, half), preferred_element_type=f32)
            out[tp, :, span] = value.T.astype(b16)
            swap(a, t).start()
            return 0

        lax.fori_loop(0, tokens // tile, step, 0)

    def swapped(a):
        await_heard((inq, ino)[a].at[1 - tp], swap_r.at[a])

    def norm(a, c, scatter):
        first, second, first_out, second_out, n_out = (
            (fq, sq, nfq_ref, nsq_ref, nq_ref), (fo, so, nfo_ref, nso_ref, no_ref)
        )[a]
        span = pl.ds(c * scatter.width, scatter.width)
        p = scatter.final(c)
        first_next = beta_first * first[:, span] + (1.0 - beta_first) * p
        second_next = beta_second * second[:, span] + (1.0 - beta_second) * p * p
        normed = first_next / jnp.sqrt(second_next)
        first_out[:, span] = first_next
        second_out[:, span] = second_next
        n_out[mine, :, span] = normed.astype(b16)

    def expand(a, first, last):
        n_ref, h_ref, u_ref = ((nq_ref, hq_ref, uq_ref), (no_ref, ho_ref, uo_ref))[a]
        rank = n_ref.shape[0] * n_ref.shape[1]
        wide = 256
        slot = pl.ds(a * 128, 128)

        def step(i, _):
            span = pl.ds(pl.multiple_of(i * wide, wide), wide)
            value = n_ref[:, :, span].reshape(rank, wide)
            u_ref[:, span] = jnp.dot(h_ref[...].reshape(-1, rank), value, preferred_element_type=f32)
            square = value.astype(f32) * value.astype(f32)
            square = square[:, :128] + square[:, 128:]
            tot_ref[0, :, slot] = tot_ref[0, :, slot] + jnp.sum(square.reshape(-1, 8, 128), axis=0)
            return 0

        lax.fori_loop(first // wide, last // wide, step, 0)

    copies[4].wait()
    project(1)
    turn(3)
    weights.tick(10)
    copies[5].wait()
    swapped(1)
    chunks = sum_o.chunks
    quarter = chunks // 4
    for c in range(chunks):
        sum_o.compute(c, ino, co)
        if c < 2 * quarter:
            sum_o.send(c)
        if c == 2 * quarter:
            turn(1)
            weights.tick(4)
    turn(len(queue))
    keep(1)
    weights.tick(2)

    def group(i):
        return range(i * quarter, (i + 1) * quarter)

    for c in group(0):
        sum_o.middle(c)
    for c in group(2):
        sum_o.send(c)
    weights.tick(2)
    for c in group(1):
        sum_o.middle(c)
    for c in group(3):
        sum_o.send(c)
    weights.tick(2)
    for copy in copies[6:]:
        copy.wait()
    basis_q.finish()
    project(0)
    for c in group(0):
        sum_o.cross(c)
    for c in group(2):
        sum_o.middle(c)
    swapped(0)
    for c in range(sum_q.chunks):
        sum_q.compute(c, inq, cq)
        sum_q.send(c)
    def cross(i):
        for c in group(i):
            sum_o.cross(c)

    def onward(i, turn):
        for c in group(i):
            sum_o.onward(c, turn)

    def both(i):
        for k in (i, i + 1):
            for c in group(k):
                norm(1, c, sum_o)

    cross(1)
    onward(0, 0)
    weights.tick(1)
    for c in group(3):
        sum_o.middle(c)
    cross(2)
    onward(1, 0)
    onward(0, 1)
    weights.tick(1)
    cross(3)
    onward(2, 0)
    onward(1, 1)
    weights.tick(1)
    for c in range(sum_q.chunks):
        sum_q.middle(c)
    onward(2, 1)
    for c in range(sum_q.chunks):
        sum_q.cross(c)
    both(0)
    norm_o[0].start()
    share(1)
    share(0)
    keep(0)
    both(2)
    norm_o[1].start()
    weights.tick(1)
    queue.extend(norm_o[0].head())
    turn(len(queue))
    for c in range(sum_q.chunks):
        norm(0, c, sum_q)
    norm_q.start()
    tot_ref[0] = jnp.zeros(tot_ref.shape[1:], f32)
    queue.extend(norm_o[1].head())
    turn(len(queue))
    queue.extend(norm_q.head())
    turn(len(queue))
    weights.tick(2)
    columns = no_ref.shape[2]
    first, second, last = norm_o[0].rest(), norm_o[1].rest(), norm_q.rest()
    for k in range(n + 2):
        for steps, lag in ((first, 0), (second, 1), (last, 2)):
            queue.extend(steps[k - lag : k - lag + 1] if k >= lag else [])
        turn(len(queue))
        weights.tick(2)
        if k == n:
            shared(1)
            norm_o[0].finish()
            expand(1, 0, columns // 2)
    norm_o[1].finish()
    expand(1, columns // 2, columns)
    shared(0)
    norm_q.finish()
    expand(0, 0, nq_ref.shape[2])
    pair = remote(tot_ref.at[0], tot_ref.at[1], pair_s.at[0], pair_r.at[0], (fs, rep, 1 - tp))
    pair.start()
    weights.finish()
    pair.wait()
    for a in (0, 1):
        await_sent((inq, ino)[a].at[tp], swap_s.at[a])
    for g in (basis_o, basis_q, *norm_o, norm_q, sum_o, sum_q):
        g.drain()
    weights.sent()


def advance(n, *args):
    xq, cq, xo, co, wq, wo, bq, bo, fq, sq, fo, so = args
    f32, b16 = jnp.float32, jnp.bfloat16
    shape, vmem = jax.ShapeDtypeStruct, pltpu.VMEM
    rank = bq.shape[1]
    half = rank // 2
    rows = fq.shape[0]
    width_q, width_o = cq.shape[1] // 2, co.shape[1] // 8

    def scatter(chunks, width):
        return [
            vmem((chunks, 4, n * rows, width), b16),
            vmem((chunks, 2, n * rows, width), b16),
            vmem((chunks, n * rows, width), b16),
            vmem((chunks, n * rows, width), b16),
            vmem((chunks, n * rows, width), f32),
            vmem((chunks, n * rows, width), b16),
            vmem((chunks, 2, n * rows, width), b16),
        ]

    pieces = sum(pieces_of(wq, wo))
    gather = [(), (n,), (2, n), ()]
    reduce = lambda chunks: [(5,), (chunks,), (chunks,), (chunks, 2)]
    shapes = gather * 5 + reduce(8) + reduce(2) + [(2,), (2,), (2,), (2,), (1,), (1,), (pieces, 2), (pieces, n)]
    spec = pl.BlockSpec(memory_space=pltpu.VMEM)
    return pl.pallas_call(
        functools.partial(main_kernel, n),
        out_shape=(
            shape((n * bq.shape[0], cq.shape[1]), f32),
            shape((n * bo.shape[0], co.shape[1]), f32),
            shape((n, *wq.shape), b16),
            shape((n, *wo.shape), b16),
            *[shape(a.shape, f32) for a in (fq, sq, fo, so)],
            shape((2, 8, 256), f32),
        ),
        in_specs=[pl.BlockSpec(memory_space=pltpu.HBM)] * 12,
        out_specs=(spec,) * 9,
        scratch_shapes=[vmem(a.shape, a.dtype) for a in (xq, cq, xo, co, wq, wo, fq, sq, fo, so)]
        + [vmem((4 * n, bq.shape[0], half), b16), vmem((4 * n, bo.shape[0], half), b16)]
        + [vmem((2, half, xq.shape[0]), b16), vmem((2, half, xo.shape[0]), b16)]
        + scatter(2, width_q)
        + scatter(8, width_o)
        + [vmem((4 * n, rows, a.shape[1]), b16) for a in (cq, co)]
        + [vmem((n, *a.shape), b16) for a in (bq, bo)]
        + [DMA((12,))]
        + [DMA(a) if a else DMA for a in shapes],
        compiler_params=pltpu.CompilerParams(
            collective_id=0, has_side_effects=True, vmem_limit_bytes=40 * 2**20
        ),
        name="advance",
    )(*[pltpu.with_memory_space_constraint(a, pltpu.HBM) for a in args])


def last_kernel(
    n,
    uq, uo, gwq, gwo, nfq, nsq, nfo, nso, tot,
    uq_out, uo_out, nfq_out, nsq_out, nfo_out, nso_out, cq_out, co_out,
    mq, mo, cq, co, sems,
):
    fs = lax.axis_index("fs")
    f32, b16 = jnp.float32, jnp.bfloat16
    rank = 4 * n * nfq.shape[0]
    copies = []

    def put(src, dst):
        copy = pltpu.make_async_copy(src, dst, sems.at[len(copies)])
        copy.start()
        copies.append(copy)

    for src, dst in ((nfq, nfq_out), (nsq, nsq_out), (nfo, nfo_out), (nso, nso_out)):
        put(src, dst)
    for a, (u, weights, m, c, m_hbm, c_hbm) in enumerate(
        ((uq, gwq, mq, cq, uq_out, cq_out), (uo, gwo, mo, co, uo_out, co_out))
    ):
        rows, columns = u.shape
        total = jnp.sum(tot[:, :, a * 128 : (a + 1) * 128], axis=0)
        total = jnp.sum(jnp.sum(total, axis=0, keepdims=True), axis=1, keepdims=True)
        scale = lax.rsqrt(total / (rank * 2 * columns) + small_eps)
        mine = m.shape[0]
        own = pl.ds(pl.multiple_of(fs * mine, mine), mine)
        m[...] = scale * u[own, :]
        put(m, m_hbm)
        block = min(128, rows)

        for k in range(0, rows, block):

            def step(i, _):
                span = pl.ds(pl.multiple_of(k + i * 16, 16), 16)
                value = scale * u[span, :]
                c[span, :] = (weights[span, :].astype(f32) - step_rate * value).astype(b16)
                return 0

            lax.fori_loop(0, block // 16, step, 0)
            span = pl.ds(k, block)
            put(c.at[span], c_hbm.at[span])
    for copy in copies:
        copy.wait()


def body(n, *args):
    xq, cq, xo, co, wq, wo, bq, bo, fq, sq, fo, so = args
    f32, b16 = jnp.float32, jnp.bfloat16
    uq, uo, gwq, gwo, nfq, nsq, nfo, nso, tot = advance(n, *args)
    shape, vmem = jax.ShapeDtypeStruct, pltpu.VMEM
    gwq, gwo = [a.reshape(-1, a.shape[2]) for a in (gwq, gwo)]
    outs = (
        shape(wq.shape, f32), shape(wo.shape, f32), shape(fq.shape, f32), shape(fq.shape, f32),
        shape(fo.shape, f32), shape(fo.shape, f32), shape(gwq.shape, b16), shape(gwo.shape, b16),
    )
    spec = pl.BlockSpec(memory_space=pltpu.VMEM)
    return pl.pallas_call(
        functools.partial(last_kernel, n),
        out_shape=outs,
        in_specs=[spec] * 9,
        out_specs=(pl.BlockSpec(memory_space=pl.ANY),) * 8,
        scratch_shapes=[vmem(wq.shape, f32), vmem(wo.shape, f32)]
        + [vmem(gwq.shape, b16), vmem(gwo.shape, b16)]
        + [DMA((6 + sum(-(-a.shape[0] // 128) for a in (gwq, gwo)),))],
        compiler_params=pltpu.CompilerParams(vmem_limit_bytes=20 * 2**20),
        name="update",
    )(uq, uo, gwq, gwo, nfq, nsq, nfo, nso, tot)


def solution(mesh):
    in_specs = (
        P(("fs", "rep"), None),
        P(("fs", "rep"), "tp"),
        P(("fs", "rep"), None),
        P(("fs", "rep"), "tp"),
        P(("rep", "fs"), "tp"),
        P(("rep", "fs"), "tp"),
        P(("rep", "fs"), None),
        P(("rep", "fs"), None),
        P(("rep", "fs"), "tp"),
        P(("rep", "fs"), "tp"),
        P(("rep", "fs"), "tp"),
        P(("rep", "fs"), "tp"),
    )
    out_specs = (
        P(("rep", "fs"), "tp"),
        P(("rep", "fs"), "tp"),
        P(("rep", "fs"), "tp"),
        P(("rep", "fs"), "tp"),
        P(("rep", "fs"), "tp"),
        P(("rep", "fs"), "tp"),
        P("rep", "tp"),
        P("rep", "tp"),
    )
    n = mesh.shape["fs"]
    assert mesh.shape["rep"] == 4 and mesh.shape["tp"] == 2
    return jax.shard_map(functools.partial(body, n), mesh=mesh, in_specs=in_specs, out_specs=out_specs, check_vma=False)
```

```python
import functools

import jax
import jax.numpy as jnp
from jax import lax
from jax.experimental import pallas as pl
from jax.experimental.pallas import tpu as pltpu
from jax.sharding import PartitionSpec as P

MESH = pl.DeviceIdType.MESH
DMA = pltpu.SemaphoreType.DMA

beta_first = 0.6
beta_second = 0.8
step_rate = 0.01
small_eps = 1e-06


def here():
    return lax.axis_index("fs"), lax.axis_index("rep"), lax.axis_index("tp")


def flip(rep, bit):
    if bit == 1:
        return rep + 1 - 2 * lax.rem(rep, 2)
    return lax.rem(rep + 2, 4)


def remote(src, dst, send, recv, device):
    return pltpu.make_async_remote_copy(
        src_ref=src, dst_ref=dst, send_sem=send, recv_sem=recv, device_id=device, device_id_type=MESH
    )


def greet(devices):
    barrier = pltpu.get_barrier_semaphore()
    for device in devices:
        pl.semaphore_signal(barrier, inc=1, device_id=device, device_id_type=MESH)
    pl.semaphore_wait(barrier, len(devices))


def when(present, body):
    if present is True:
        body()
    else:
        pl.when(present)(body)


def await_sent(view, sem):
    remote(view, view, sem, sem, here()).wait_send()


def await_heard(view, sem):
    remote(view, view, sem, sem, here()).wait_recv()


class Line:
    def __init__(self, n, view, send, recv):
        self.n, self.view, self.send_sem, self.recv_sem = n, view, send, recv
        self.fs, self.rep, self.tp = here()

    def outgoing(self, step, way):
        fs, n = self.fs, self.n
        if way == 0:
            block, peer = fs - step + 1, fs + 1
            present = jnp.logical_and(block >= 0, peer < n)
        else:
            block, peer = fs + step - 1, fs - 1
            present = jnp.logical_and(block < n, peer >= 0)
        block = lax.rem(block + n, n)
        peer = lax.rem(peer + n, n)
        view = self.view(block)
        return remote(view, view, self.send_sem.at[way], self.recv_sem.at[block], (peer, self.rep, self.tp)), present

    def start(self, step, part=None):
        for way in (0, 1):
            copy, present = self.outgoing(step, way)
            if part is not None:
                right = 2 * self.fs >= self.n if (way == 0) == (part == 0) else 2 * self.fs < self.n
                present = jnp.logical_and(present, right)
            when(present, copy.start)

    def arrive(self, step):
        for way in (0, 1):
            block = self.fs - step if way == 0 else self.fs + step
            present = block >= 0 if way == 0 else block < self.n
            block = lax.rem(block + self.n, self.n)
            when(present, lambda: await_heard(self.view(block), self.recv_sem.at[block]))

    def sent(self, many):
        for place in range(self.n):
            right = place + 1 if place < self.n - 1 else 0
            left = self.n - place if place > 0 else 0

            def body():
                for way, count in enumerate((right, left)):
                    if count:
                        await_sent(many(count), self.send_sem.at[way])

            pl.when(self.fs == place)(body)


class Gather:
    bits = ((1, 2), (2, 1))

    def __init__(self, n, far, view, many, send, line, one, two):
        self.far = far and n > 3
        self.n, self.view, self.many, self.send_sem = n, view, many, send
        self.line, self.one_sem, self.two_sem = line, one, two
        self.fs, self.rep, self.tp = here()

    def slots(self, step):
        if step == 0:
            return [(self.fs, True)]
        left, right = self.fs - step, self.fs + step
        rem = lambda block: lax.rem(block + self.n, self.n)
        return [(rem(left), left >= 0), (rem(right), right < self.n)]

    def each(self, step, action):
        for block, present in self.slots(step):
            when(present, lambda: action(block))

    def one(self, block, half):
        peer = flip(self.rep, self.bits[half][0])
        view = self.view(self.rep * self.n + block, half)
        return remote(view, view, self.send_sem, self.one_sem.at[half, block], (self.fs, peer, self.tp))

    def two(self, block, half, which):
        peer = flip(self.rep, self.bits[half][1])
        held = self.rep if which == 0 else flip(self.rep, self.bits[half][0])
        view = self.view(held * self.n + block, half)
        return remote(view, view, self.send_sem, self.two_sem, (self.fs, peer, self.tp))

    def launch(self, step):
        def action(block):
            for half in (0, 1):
                self.one(block, half).start()
            for half in (0, 1):
                self.two(block, half, 0).start()

        self.each(step, action)

    def start(self):
        for step in range(1, self.n - 1 if self.far else self.n):
            for peer, present in self.slots(step):
                when(present, lambda: self.along(self.fs, peer))
        self.launch(0)

    def along(self, block, peer):
        view = self.view(self.rep * self.n + block, None)
        remote(view, view, self.send_sem, self.line.at[block], (peer, self.rep, self.tp)).start()

    def arrive(self, step):
        self.each(step, lambda block: await_heard(self.view(self.rep * self.n + block, None), self.line.at[block]))
        if self.far and step == self.n - 2:
            for place, block, peer in ((1, self.n - 1, 0), (self.n - 2, 0, self.n - 1)):
                pl.when(self.fs == place)(lambda: self.along(block, peer))
        self.launch(step)

    def relay(self, step):
        def action(block):
            for half in (0, 1):
                peer = flip(self.rep, self.bits[half][0])
                await_heard(self.view(peer * self.n + block, half), self.one_sem.at[half, block])
                self.two(block, half, 1).start()

        self.each(step, action)

    def events(self):
        n = self.n
        todo = [(self.relay, 0)]
        for step in range(1, n):
            todo.append((self.arrive, step))
            if step >= 2:
                todo.append((self.relay, step - 1))
        return todo + ([(self.relay, n - 1)] if n > 1 else [])

    def head(self):
        return [(self.relay, 0)] + [(self.arrive, step) for step in range(1, self.n - 1)]

    def rest(self):
        n = self.n
        return [(self.relay, 1), (self.arrive, n - 1)] + [(self.relay, step) for step in range(2, n)]

    def finish(self):
        await_heard(self.many(2 * self.n), self.two_sem)

    def drain(self):
        n = self.n
        for place in range(n):
            count = 4 * n - 1
            if self.far:
                count += -1 if place in (0, n - 1) else 1 if place in (1, n - 2) else 0
            pl.when(self.fs == place)(lambda: await_sent(self.many(count), self.send_sem))


class Scatter:
    def __init__(self, n, direct, part, one, mid, two, total, out, late, send, one_sem, two_sem, line_sem):
        self.n, self.part, self.heard, self.mid_ref, self.two = n, part, one, mid, two
        self.total, self.out, self.late = total, out, late
        self.send_sem, self.one_sem, self.two_sem, self.line_sem = send, one_sem, two_sem, line_sem
        self.fs, self.rep, self.tp = here()
        self.chunks, _, group, self.width = part.shape
        self.rows = group // n
        self.direct = direct

    def peers(self, c):
        first, second = ((1, 2), (2, 1))[c % 2]
        return flip(self.rep, first), flip(self.rep, second), second

    def compute(self, c, inner, cotangent):
        tile = min(256, self.width)
        rank = inner.shape[0] * inner.shape[1]

        def step(i, _):
            span = pl.ds(pl.multiple_of(c * self.width + i * tile, tile), tile)
            value = jnp.dot(
                inner[...].reshape(rank, -1), cotangent[:, span], preferred_element_type=jnp.float32
            )
            here_span = pl.ds(pl.multiple_of(i * tile, tile), tile)
            self.part[c, :, :, here_span] = value.astype(jnp.bfloat16).reshape(4, -1, tile)
            return 0

        lax.fori_loop(0, self.width // tile, step, 0)

    def send(self, c):
        near, _, second = self.peers(c)
        for slot, group in ((1, flip(near, second)), (0, near)):
            remote(
                self.part.at[c, group], self.heard.at[c, slot], self.send_sem.at[0], self.one_sem.at[c],
                (self.fs, near, self.tp),
            ).start()

    def middle(self, c):
        f32 = jnp.float32
        _, far, _ = self.peers(c)
        await_heard(self.heard.at[c], self.one_sem.at[c])
        value = self.part[c, far].astype(f32) + self.heard[c, 1].astype(f32)
        self.mid_ref[c] = value.astype(jnp.bfloat16)
        remote(
            self.mid_ref.at[c], self.two.at[c], self.send_sem.at[1], self.two_sem.at[c], (self.fs, far, self.tp)
        ).start()
        self.total[c] = self.part[c, self.rep].astype(f32) + self.heard[c, 0].astype(f32)

    def sums(self, c, rows):
        return self.total[c, rows, :] + self.two[c, rows, :].astype(jnp.float32)

    def stream(self, c, place, way, heard):
        n, r = self.n, self.rows
        rows = pl.ds((place + 1) * r, (n - 1 - place) * r) if way == 0 else pl.ds(0, place * r)
        value = self.sums(c, rows)
        if heard:
            value = value + self.late[c, way, rows, :].astype(jnp.float32)
        self.out[c, rows, :] = value.astype(jnp.bfloat16)
        peer = (place + 1 if way == 0 else place - 1, self.rep, self.tp)
        remote(
            self.out.at[c, rows], self.late.at[c, way, rows], self.send_sem.at[2 + way],
            self.line_sem.at[c, way], peer,
        ).start()

    def hear(self, c, place, way):
        n, r = self.n, self.rows
        rows = pl.ds(place * r, (n - place) * r) if way == 0 else pl.ds(0, (place + 1) * r)
        await_heard(self.late.at[c, way, rows], self.line_sem.at[c, way])

    def cross(self, c):
        await_heard(self.two.at[c], self.two_sem.at[c])
        if c >= self.direct:
            r = self.rows
            mine = pl.ds(pl.multiple_of(self.fs * r, r), r)
            for j in range(1, self.n):
                f = lax.rem(self.fs + j, self.n)
                rows = pl.ds(pl.multiple_of(f * r, r), r)
                self.out[c, rows, :] = self.sums(c, rows).astype(jnp.bfloat16)
                remote(
                    self.out.at[c, rows], self.late.at[c, 0, mine], self.send_sem.at[4],
                    self.line_sem.at[c, 0], (f, self.rep, self.tp),
                ).start()
            return
        for place, way in ((0, 0), (self.n - 1, 1)):
            pl.when(self.fs == place)(lambda: self.stream(c, place, way, False))

    def onward(self, c, turn):
        for place in range(1, self.n - 1):
            way = turn if 2 * place < self.n else 1 - turn

            def body():
                self.hear(c, place, way)
                self.stream(c, place, way, True)

            pl.when(self.fs == place)(body)

    def final(self, c):
        n, r = self.n, self.rows
        own = pl.ds(pl.multiple_of(self.fs * r, r), r)
        if c >= self.direct:
            value = self.sums(c, own)
            await_heard(self.late.at[c, 0, pl.ds(0, (n - 1) * r)], self.line_sem.at[c, 0])
            for j in range(1, n):
                f = lax.rem(self.fs + j, n)
                value = value + self.late[c, 0, pl.ds(pl.multiple_of(f * r, r), r), :].astype(jnp.float32)
            return value
        for place, way in ((0, 1), (n - 1, 0)):
            pl.when(self.fs == place)(lambda: self.hear(c, place, way))
        self.total[c, own, :] = self.sums(c, own)
        for way, present in ((0, self.fs > 0), (1, self.fs < n - 1)):

            def body():
                self.total[c, own, :] = self.total[c, own, :] + self.late[c, way, own, :].astype(jnp.float32)

            pl.when(present)(body)
        return self.total[c, own, :]

    def drain(self):
        await_sent(self.heard, self.send_sem.at[0])
        await_sent(self.mid_ref, self.send_sem.at[1])
        n, r = self.n, self.rows
        if self.direct < self.chunks:
            direct = pl.ds(self.direct, self.chunks - self.direct)
            await_sent(self.out.at[direct, pl.ds(0, (n - 1) * r)], self.send_sem.at[4])
        if self.direct == 0:
            return
        for place in range(n):

            def body():
                for way, count in ((0, n - 1 - place), (1, place)):
                    if count:
                        rows = pl.ds(0, count * r)
                        await_sent(self.out.at[pl.ds(0, self.direct), rows], self.send_sem.at[2 + way])

            pl.when(self.fs == place)(body)


class Weights:
    def __init__(self, n, views, many, send, recv):
        self.lines = [Line(n, view, send.at[a], recv.at[i]) for i, (a, view) in enumerate(views)]
        self.last = [Line(n, None, send.at[a], None) for a in range(len(many))]
        self.n, self.many = n, many
        self.todo = [(step, line, None) for step in range(1, n) for line in self.lines]

    def early(self, count):
        for k in range(count):
            step, line, _ = self.todo[k]
            line.start(step, 0)
            self.todo[k] = (step, line, 1)

    def tick(self, count):
        for _ in range(count):
            if self.todo:
                step, line, part = self.todo.pop(0)
                if step > 1:
                    line.arrive(step - 1)
                line.start(step, part)

    def finish(self):
        self.tick(len(self.todo))
        for line in self.lines:
            line.arrive(self.n - 1)

    def sent(self):
        for line, many in zip(self.last, self.many):
            line.sent(many)


def pieces_of(*refs):
    return [min(most, ref.shape[-2] // 8) for most, ref in zip((4, 8), refs)]


def main_kernel(
    n,
    xq_hbm, cq_hbm, xo_hbm, co_hbm, wq_hbm, wo_hbm, bq_hbm, bo_hbm, fq_hbm, sq_hbm, fo_hbm, so_hbm,
    uq_ref, uo_ref, gwq_ref, gwo_ref, nfq_ref, nsq_ref, nfo_ref, nso_ref, tot_ref,
    xq, cq, xo, co, wq, wo, fq, sq, fo, so, gbq, gbo, inq, ino,
    part_q, one_q, mid_q, two_q, total_q, out_q, late_q,
    part_o, one_o, mid_o, two_o, total_o, out_o, late_o,
    nq_ref, no_ref, hq_ref, ho_ref, local, *sems,
):
    fs, rep, tp = here()
    mine = rep * n + fs
    f32, b16 = jnp.float32, jnp.bfloat16
    sems = list(sems)
    take = lambda count: [sems.pop(0) for _ in range(count)]

    half = bq_hbm.shape[1] // 2
    own = pl.ds(pl.multiple_of(tp * half, half), half)
    copies = [
        pltpu.make_async_copy(src, dst, local.at[i])
        for i, (src, dst) in enumerate(
            [
                (bo_hbm.at[:, own], gbo.at[mine]), (bq_hbm.at[:, own], gbq.at[mine]),
                (wq_hbm, wq), (wo_hbm, wo), (xo_hbm, xo), (co_hbm, co), (xq_hbm, xq), (cq_hbm, cq),
                (fo_hbm, fo), (so_hbm, so), (fq_hbm, fq), (sq_hbm, sq),
            ]
        )
    ]
    for copy in copies:
        copy.start()
    copies[0].wait()
    copies[1].wait()
    peers = [(lax.rem(fs + k, n), rep, tp) for k in range(1, n)]
    peers += [(fs, flip(rep, bit), tp) for bit in (1, 2)] + [(fs, rep, 1 - tp)]
    greet(peers)

    def rows_view(ref):
        rows = ref.shape[1] // 2

        def view(block, part):
            return ref.at[block] if part is None else ref.at[block, pl.ds(part * rows, rows)]

        return view, lambda count: ref.at[pl.ds(0, count)]

    def cols_view(ref, index=0, count=1):
        cols = ref.shape[2] // (2 * count)

        def view(block, part):
            start, size = (0, 2 * cols) if part is None else (part * cols, cols)
            return ref.at[block, :, pl.ds(index * 2 * cols + start, size)]

        return view, lambda k: ref.at[pl.ds(0, k), :, pl.ds(index * 2 * cols, 2 * cols)]

    basis_o = Gather(n, False, *rows_view(gbo), *take(4))
    basis_q = Gather(n, False, *rows_view(gbq), *take(4))
    norm_o = [Gather(n, True, *cols_view(no_ref, i, 2), *take(4)) for i in range(2)]
    norm_q = Gather(n, True, *cols_view(nq_ref), *take(4))
    sum_o = Scatter(n, 3 * part_o.shape[0] // 4, part_o, one_o, mid_o, two_o, total_o, out_o, late_o, *take(4))
    sum_q = Scatter(n, 0, part_q, one_q, mid_q, two_q, total_q, out_q, late_q, *take(4))
    swap_s, swap_r, share_s, share_r, pair_s, pair_r, weight_s, weight_r = take(8)

    views, many = [], []
    for a, (ref, pieces) in enumerate(zip((gwq_ref, gwo_ref), pieces_of(gwq_ref, gwo_ref))):
        rows = ref.shape[1] // pieces
        many.append(lambda k, ref=ref: ref.at[pl.ds(0, k)])
        for p in range(pieces):
            views.append((a, lambda b, ref=ref, p=p, rows=rows: ref.at[b, pl.ds(p * rows, rows)]))
    weights = Weights(n, views, many, weight_s, weight_r)

    basis_o.start()
    basis_q.start()
    copies[2].wait()
    copies[3].wait()
    gwq_ref[fs] = wq[...].astype(b16)
    gwo_ref[fs] = wo[...].astype(b16)
    weights.early(4)

    queue = basis_q.events()

    def turn(count):
        for _ in range(count):
            if queue:
                action, step = queue.pop(0)
                action(step)

    for step in range(1, n):
        basis_o.arrive(step)
        basis_o.relay(step - 1)
        if step == 2:
            turn(1)
    basis_o.relay(n - 1)
    turn(1)
    basis_o.finish()

    def share(a):
        gb, out = ((gbq, hq_ref), (gbo, ho_ref))[a]
        for f in range(n):
            view = out.at[f, :, own]
            remote(gb.at[rep * n + f], view, share_s.at[a], share_r.at[a], (fs, rep, 1 - tp)).start()

    def shared(a):
        gb, out = ((gbq, hq_ref), (gbo, ho_ref))[a]
        other = pl.ds(pl.multiple_of((1 - tp) * half, half), half)
        await_heard(out.at[:, :, other], share_r.at[a])
        await_sent(gb.at[pl.ds(0, n)], share_s.at[a])

    def keep(a):
        gb, out = ((gbq, hq_ref), (gbo, ho_ref))[a]
        for f in range(n):
            out[f, :, own] = gb[rep * n + f]

    tokens = xq.shape[0]
    tile = min(512, tokens)

    def swap(a, t):
        ref = (inq, ino)[a]
        view = ref.at[tp, :, pl.ds(pl.multiple_of(t * tile, tile), tile)]
        return remote(view, view, swap_s.at[a], swap_r.at[a], (fs, rep, 1 - tp))

    def project(a):
        x, gb, out = ((xq, gbq, inq), (xo, gbo, ino))[a]

        def step(t, _):
            span = pl.ds(pl.multiple_of(t * tile, tile), tile)
            value = jnp.dot(x[span, :], gb[...].reshape(-1, half), preferred_element_type=f32)
            out[tp, :, span] = value.T.astype(b16)
            swap(a, t).start()
            return 0

        lax.fori_loop(0, tokens // tile, step, 0)

    def swapped(a):
        await_heard((inq, ino)[a].at[1 - tp], swap_r.at[a])

    def norm(a, c, scatter):
        first, second, first_out, second_out, n_out = (
            (fq, sq, nfq_ref, nsq_ref, nq_ref), (fo, so, nfo_ref, nso_ref, no_ref)
        )[a]
        span = pl.ds(c * scatter.width, scatter.width)
        p = scatter.final(c)
        first_next = beta_first * first[:, span] + (1.0 - beta_first) * p
        second_next = beta_second * second[:, span] + (1.0 - beta_second) * p * p
        normed = first_next / jnp.sqrt(second_next)
        first_out[:, span] = first_next
        second_out[:, span] = second_next
        n_out[mine, :, span] = normed.astype(b16)

    def expand(a, first, last):
        n_ref, h_ref, u_ref = ((nq_ref, hq_ref, uq_ref), (no_ref, ho_ref, uo_ref))[a]
        rank = n_ref.shape[0] * n_ref.shape[1]
        wide = 256
        slot = pl.ds(a * 128, 128)

        def step(i, _):
            span = pl.ds(pl.multiple_of(i * wide, wide), wide)
            value = n_ref[:, :, span].reshape(rank, wide)
            u_ref[:, span] = jnp.dot(h_ref[...].reshape(-1, rank), value, preferred_element_type=f32)
            square = value.astype(f32) * value.astype(f32)
            square = square[:, :128] + square[:, 128:]
            tot_ref[0, :, slot] = tot_ref[0, :, slot] + jnp.sum(square.reshape(-1, 8, 128), axis=0)
            return 0

        lax.fori_loop(first // wide, last // wide, step, 0)

    copies[4].wait()
    project(1)
    turn(3)
    weights.tick(10)
    copies[5].wait()
    swapped(1)
    chunks = sum_o.chunks
    quarter = chunks // 4
    for c in range(chunks):
        sum_o.compute(c, ino, co)
        if c < 2 * quarter:
            sum_o.send(c)
        if c == 2 * quarter:
            turn(1)
            weights.tick(4)
    turn(len(queue))
    keep(1)
    weights.tick(2)

    def group(i):
        return range(i * quarter, (i + 1) * quarter)

    for c in group(0):
        sum_o.middle(c)
    for c in group(2):
        sum_o.send(c)
    weights.tick(2)
    for c in group(1):
        sum_o.middle(c)
    for c in group(3):
        sum_o.send(c)
    weights.tick(2)
    for copy in copies[6:]:
        copy.wait()
    basis_q.finish()
    project(0)
    for c in group(0):
        sum_o.cross(c)
    for c in group(2):
        sum_o.middle(c)
    swapped(0)
    for c in range(sum_q.chunks):
        sum_q.compute(c, inq, cq)
        sum_q.send(c)
    def cross(i):
        for c in group(i):
            sum_o.cross(c)

    def onward(i, turn):
        for c in group(i):
            sum_o.onward(c, turn)

    def both(i):
        for k in (i, i + 1):
            for c in group(k):
                norm(1, c, sum_o)

    cross(1)
    onward(0, 0)
    weights.tick(1)
    for c in group(3):
        sum_o.middle(c)
    cross(2)
    onward(1, 0)
    onward(0, 1)
    weights.tick(1)
    cross(3)
    onward(2, 0)
    onward(1, 1)
    weights.tick(1)
    for c in range(sum_q.chunks):
        sum_q.middle(c)
    onward(2, 1)
    for c in range(sum_q.chunks):
        sum_q.cross(c)
    both(0)
    norm_o[0].start()
    share(1)
    share(0)
    keep(0)
    both(2)
    norm_o[1].start()
    weights.tick(2)
    queue.extend(norm_o[0].head())
    turn(len(queue))
    for c in range(sum_q.chunks):
        norm(0, c, sum_q)
    norm_q.start()
    tot_ref[0] = jnp.zeros(tot_ref.shape[1:], f32)
    queue.extend(norm_o[1].head())
    turn(len(queue))
    queue.extend(norm_q.head())
    turn(len(queue))
    weights.tick(2)
    columns = no_ref.shape[2]
    first, second, last = norm_o[0].rest(), norm_o[1].rest(), norm_q.rest()
    for k in range(n + 2):
        for steps, lag in ((first, 0), (second, 1), (last, 2)):
            queue.extend(steps[k - lag : k - lag + 1] if k >= lag else [])
        turn(len(queue))
        weights.tick(2)
        if k == n:
            shared(1)
            norm_o[0].finish()
            expand(1, 0, columns // 2)
    norm_o[1].finish()
    expand(1, columns // 2, columns)
    shared(0)
    norm_q.finish()
    expand(0, 0, nq_ref.shape[2])
    pair = remote(tot_ref.at[0], tot_ref.at[1], pair_s.at[0], pair_r.at[0], (fs, rep, 1 - tp))
    pair.start()
    weights.finish()
    pair.wait()
    for a in (0, 1):
        await_sent((inq, ino)[a].at[tp], swap_s.at[a])
    for g in (basis_o, basis_q, *norm_o, norm_q, sum_o, sum_q):
        g.drain()
    weights.sent()


def advance(n, *args):
    xq, cq, xo, co, wq, wo, bq, bo, fq, sq, fo, so = args
    f32, b16 = jnp.float32, jnp.bfloat16
    shape, vmem = jax.ShapeDtypeStruct, pltpu.VMEM
    rank = bq.shape[1]
    half = rank // 2
    rows = fq.shape[0]
    width_q, width_o = cq.shape[1] // 2, co.shape[1] // 8

    def scatter(chunks, width):
        return [
            vmem((chunks, 4, n * rows, width), b16),
            vmem((chunks, 2, n * rows, width), b16),
            vmem((chunks, n * rows, width), b16),
            vmem((chunks, n * rows, width), b16),
            vmem((chunks, n * rows, width), f32),
            vmem((chunks, n * rows, width), b16),
            vmem((chunks, 2, n * rows, width), b16),
        ]

    pieces = sum(pieces_of(wq, wo))
    gather = [(), (n,), (2, n), ()]
    reduce = lambda chunks: [(5,), (chunks,), (chunks,), (chunks, 2)]
    shapes = gather * 5 + reduce(8) + reduce(2) + [(2,), (2,), (2,), (2,), (1,), (1,), (2, 2), (pieces, n)]
    spec = pl.BlockSpec(memory_space=pltpu.VMEM)
    return pl.pallas_call(
        functools.partial(main_kernel, n),
        out_shape=(
            shape((n * bq.shape[0], cq.shape[1]), f32),
            shape((n * bo.shape[0], co.shape[1]), f32),
            shape((n, *wq.shape), b16),
            shape((n, *wo.shape), b16),
            *[shape(a.shape, f32) for a in (fq, sq, fo, so)],
            shape((2, 8, 256), f32),
        ),
        in_specs=[pl.BlockSpec(memory_space=pltpu.HBM)] * 12,
        out_specs=(spec,) * 9,
        scratch_shapes=[vmem(a.shape, a.dtype) for a in (xq, cq, xo, co, wq, wo, fq, sq, fo, so)]
        + [vmem((4 * n, bq.shape[0], half), b16), vmem((4 * n, bo.shape[0], half), b16)]
        + [vmem((2, half, xq.shape[0]), b16), vmem((2, half, xo.shape[0]), b16)]
        + scatter(2, width_q)
        + scatter(8, width_o)
        + [vmem((4 * n, rows, a.shape[1]), b16) for a in (cq, co)]
        + [vmem((n, *a.shape), b16) for a in (bq, bo)]
        + [DMA((12,))]
        + [DMA(a) if a else DMA for a in shapes],
        compiler_params=pltpu.CompilerParams(
            collective_id=0, has_side_effects=True, vmem_limit_bytes=40 * 2**20
        ),
        name="advance",
    )(*[pltpu.with_memory_space_constraint(a, pltpu.HBM) for a in args])


def last_kernel(
    n,
    uq, uo, gwq, gwo, nfq, nsq, nfo, nso, tot,
    uq_out, uo_out, nfq_out, nsq_out, nfo_out, nso_out, cq_out, co_out,
    mq, mo, cq, co, sems,
):
    fs = lax.axis_index("fs")
    f32, b16 = jnp.float32, jnp.bfloat16
    rank = 4 * n * nfq.shape[0]
    copies = []

    def put(src, dst):
        copy = pltpu.make_async_copy(src, dst, sems.at[len(copies)])
        copy.start()
        copies.append(copy)

    for src, dst in ((nfq, nfq_out), (nsq, nsq_out), (nfo, nfo_out), (nso, nso_out)):
        put(src, dst)
    for a, (u, weights, m, c, m_hbm, c_hbm) in enumerate(
        ((uq, gwq, mq, cq, uq_out, cq_out), (uo, gwo, mo, co, uo_out, co_out))
    ):
        rows, columns = u.shape
        total = jnp.sum(tot[:, :, a * 128 : (a + 1) * 128], axis=0)
        total = jnp.sum(jnp.sum(total, axis=0, keepdims=True), axis=1, keepdims=True)
        scale = lax.rsqrt(total / (rank * 2 * columns) + small_eps)
        mine = m.shape[0]
        own = pl.ds(pl.multiple_of(fs * mine, mine), mine)
        m[...] = scale * u[own, :]
        put(m, m_hbm)
        block = min(128, rows)

        for k in range(0, rows, block):

            def step(i, _):
                span = pl.ds(pl.multiple_of(k + i * 16, 16), 16)
                value = scale * u[span, :]
                c[span, :] = (weights[span, :].astype(f32) - step_rate * value).astype(b16)
                return 0

            lax.fori_loop(0, block // 16, step, 0)
            span = pl.ds(k, block)
            put(c.at[span], c_hbm.at[span])
    for copy in copies:
        copy.wait()


def body(n, *args):
    xq, cq, xo, co, wq, wo, bq, bo, fq, sq, fo, so = args
    f32, b16 = jnp.float32, jnp.bfloat16
    uq, uo, gwq, gwo, nfq, nsq, nfo, nso, tot = advance(n, *args)
    shape, vmem = jax.ShapeDtypeStruct, pltpu.VMEM
    gwq, gwo = [a.reshape(-1, a.shape[2]) for a in (gwq, gwo)]
    outs = (
        shape(wq.shape, f32), shape(wo.shape, f32), shape(fq.shape, f32), shape(fq.shape, f32),
        shape(fo.shape, f32), shape(fo.shape, f32), shape(gwq.shape, b16), shape(gwo.shape, b16),
    )
    spec = pl.BlockSpec(memory_space=pltpu.VMEM)
    return pl.pallas_call(
        functools.partial(last_kernel, n),
        out_shape=outs,
        in_specs=[spec] * 9,
        out_specs=(pl.BlockSpec(memory_space=pl.ANY),) * 8,
        scratch_shapes=[vmem(wq.shape, f32), vmem(wo.shape, f32)]
        + [vmem(gwq.shape, b16), vmem(gwo.shape, b16)]
        + [DMA((6 + sum(-(-a.shape[0] // 128) for a in (gwq, gwo)),))],
        compiler_params=pltpu.CompilerParams(vmem_limit_bytes=20 * 2**20),
        name="update",
    )(uq, uo, gwq, gwo, nfq, nsq, nfo, nso, tot)


def solution(mesh):
    in_specs = (
        P(("fs", "rep"), None),
        P(("fs", "rep"), "tp"),
        P(("fs", "rep"), None),
        P(("fs", "rep"), "tp"),
        P(("rep", "fs"), "tp"),
        P(("rep", "fs"), "tp"),
        P(("rep", "fs"), None),
        P(("rep", "fs"), None),
        P(("rep", "fs"), "tp"),
        P(("rep", "fs"), "tp"),
        P(("rep", "fs"), "tp"),
        P(("rep", "fs"), "tp"),
    )
    out_specs = (
        P(("rep", "fs"), "tp"),
        P(("rep", "fs"), "tp"),
        P(("rep", "fs"), "tp"),
        P(("rep", "fs"), "tp"),
        P(("rep", "fs"), "tp"),
        P(("rep", "fs"), "tp"),
        P("rep", "tp"),
        P("rep", "tp"),
    )
    n = mesh.shape["fs"]
    assert mesh.shape["rep"] == 4 and mesh.shape["tp"] == 2
    return jax.shard_map(functools.partial(body, n), mesh=mesh, in_specs=in_specs, out_specs=out_specs, check_vma=False)
```
